32 devices in a mesh: fs: 8 (over z, y), tp: 4 (over x, core).
Axes of the slice: x: 2, y: 2, z: 4, core: 2. Of those that a mesh axis runs over, the one named last changes fastest.
Arguments:
- inputs: bfloat16 [4096, 2112], P('fs', 'tp'), may hold values from -6 to 6
- w_conv_up: bfloat16 [2112, 2816], P('fs', 'tp'), may hold values from -0.125 to 0.125
- w_gate_up: bfloat16 [2112, 2816], P('fs', 'tp'), may hold values from -0.125 to 0.125
- w_down: bfloat16 [2816, 2112], P('tp', 'fs'), may hold values from -0.109375 to 0.109375
- taps: float32 [3, 2816], replicated, may hold values from -3 to 3
- conv_bias: float32 [2816], replicated, may hold values from -3 to 3
- cotangent: bfloat16 [4096, 2112], P('fs', 'tp'), may hold values from -6 to 6
Outputs:
- grad_inputs: bfloat16 [4096, 2112], P('fs', 'tp')
- grad_conv_up: float32 [2112, 2816], P('fs', 'tp')
- unit_norms: float32 [2816], P('tp')
- grad_taps: float32 [3, 2816], replicated
- grad_bias: float32 [2816], replicated
The draws below stay inside these ranges and needn't reach their ends.
All inputs are finite; a program needn't handle non-finite values.
Results may differ from the reference program's by a relative error of at most 0.018.
Values may be sent and summed in bfloat16 or wider, within the bound.
A program may use at most 64 MiB of HBM per device.

```python
import math
import jax
import jax.numpy as jnp
from jax import lax

D = 2112
FF = 2816
TAPS = 3
TOKENS = 4096
N_TP = 4


def with_spikes(entries, key, source, target, shards_of, factor):
    def block_of(dim):
        return (jnp.arange(entries.shape[dim]) // (entries.shape[dim] // shards_of)).reshape((-1,) + (1,) * (entries.ndim - 1 - dim))

    near = jax.random.permutation(key, shards_of)[block_of(target)]
    other_side = (block_of(target) + shards_of // 2) % shards_of
    return jnp.where((block_of(source) == near) | (block_of(source) == other_side), factor * entries, entries)


def shard_levels(key, extent, split, smallest, high):
    def one(dim, blocks):
        steps = jax.random.uniform(jax.random.fold_in(jax.random.fold_in(key, 6), dim), (blocks,), jnp.float32, smallest / len(split), high / len(split))
        return jnp.repeat(jnp.exp(steps), extent[dim] // blocks).reshape((-1,) + (1,) * (len(extent) - dim - 1))

    level = one(*split[0])
    for cut in split[1:]:
        level = level * one(*cut)
    return level


def gaussian(own_key, dims, scale, reach, cuts=(), kind=jnp.bfloat16):
    level = shard_levels(own_key, dims, cuts, -0.22, 0.18) if cuts else 1.0
    result = jax.random.normal(own_key, dims, jnp.float32) * scale * level
    return jnp.minimum(jnp.maximum(result, -reach), reach).astype(kind)


def heavy_noise(stream_key, extent, deviation, limit, cuts, heavy, held_as=jnp.bfloat16):
    entries = deviation * jax.random.normal(stream_key, extent, jnp.float32)
    if cuts:
        entries = entries * shard_levels(stream_key, extent, cuts, -0.22, 0.18)
    return jnp.clip(with_spikes(entries, jax.random.fold_in(stream_key, 3), *heavy), -limit, limit).astype(held_as)


def setup_inputs(seed: int = 0) -> dict:
    key_list = jax.random.split(jax.random.key(seed), 8)
    return {
        "inputs": heavy_noise(key_list[0], (TOKENS, D), 1.0, 6.0, ((0, 8), (1, 4)), (0, 1, 8, 2.0)),
        "w_conv_up": gaussian(key_list[1], (D, FF), D ** -0.5, 0.125, ((0, 8), (1, 4))),
        "w_gate_up": gaussian(key_list[2], (D, FF), D ** -0.5, 0.125, ((0, 8), (1, 4))),
        "w_down": gaussian(key_list[3], (FF, D), FF ** -0.5, 0.109375, ((0, 4), (1, 8))),
        "taps": gaussian(key_list[4], (TAPS, FF), 0.6, 3.0, (), jnp.float32),
        "conv_bias": gaussian(key_list[5], (FF,), 0.5, 3.0, (), jnp.float32),
        "cotangent": gaussian(key_list[6], (TOKENS, D), 1.0, 6.0, ((0, 8), (1, 4))),
    }


def gelu_parts(value):
    normal_cdf = 0.5 * (1.0 + jax.scipy.special.erf(value / math.sqrt(2.0)))
    density = jnp.exp(-0.5 * value * value) / math.sqrt(2.0 * math.pi)
    return (value * normal_cdf, normal_cdf + value * density)

def reference(inputs, w_conv_up, w_gate_up, w_down, taps, conv_bias, cotangent):
    span = TAPS - 1
    rows = inputs.shape[0]
    up_a = jnp.dot(inputs, w_conv_up, preferred_element_type=jnp.float32).astype(jnp.bfloat16)
    up_b = jnp.dot(inputs, w_gate_up, preferred_element_type=jnp.float32).astype(jnp.bfloat16)
    extended = jnp.concatenate([jnp.zeros((span, FF), jnp.float32), up_a.astype(jnp.float32)], 0)
    conv_out = conv_bias[None, :] + sum((taps[i][None, :] * extended[i:i + rows] for i in range(TAPS)))
    d_hidden = jnp.dot(cotangent, w_down.T, preferred_element_type=jnp.float32).astype(jnp.bfloat16)
    gelu_value, gelu_slope = gelu_parts(conv_out)
    d_conv = d_hidden.astype(jnp.float32) * up_b.astype(jnp.float32) * gelu_slope
    d_up_b = (d_hidden.astype(jnp.float32) * gelu_value).astype(jnp.bfloat16)
    d_extended = jnp.concatenate([d_conv, jnp.zeros((span, FF), jnp.float32)], 0)
    d_up_a = sum((taps[i][None, :] * d_extended[span - i:span - i + rows] for i in range(TAPS))).astype(jnp.bfloat16)
    grad_taps = jnp.stack([lax.optimization_barrier(jnp.sum(d_conv * extended[i:i + rows], axis=0)) for i in range(TAPS)], 0)
    grad_bias = lax.optimization_barrier(jnp.sum(d_conv, axis=0))
    group = FF // N_TP
    total = jnp.zeros((rows, D), jnp.float32)
    for k in range(N_TP):
        lo = k * group
        part = jnp.dot(d_up_a[:, lo:lo + group], w_conv_up[:, lo:lo + group].T, preferred_element_type=jnp.float32)
        part = part + jnp.dot(d_up_b[:, lo:lo + group], w_gate_up[:, lo:lo + group].T, preferred_element_type=jnp.float32)
        total = total + part.astype(jnp.bfloat16).astype(jnp.float32)
    grad_inputs = total.astype(jnp.bfloat16)
    grad_conv_up = jnp.dot(inputs.T, d_up_a, preferred_element_type=jnp.float32)
    unit_norms = lax.optimization_barrier(jnp.sum(grad_conv_up * grad_conv_up, axis=0))
    return (grad_inputs, grad_conv_up, unit_norms, grad_taps, grad_bias)
```

```python
import functools
import math

import jax
import jax.numpy as jnp
from jax import lax
from jax.experimental import pallas as pl
from jax.experimental.pallas import tpu as pltpu
from jax.sharding import PartitionSpec as P

TAPS = 3
LANES = 128
MESH = pl.DeviceIdType.MESH
VMEM = pl.BlockSpec(memory_space=pltpu.VMEM)
ANY = pl.BlockSpec(memory_space=pl.ANY)


def shifted(block, axis, distance):
    devices = range(lax.axis_size(axis))
    route = [(i - distance, i) for i in devices if i - distance in devices]
    return lax.ppermute(block, axis, route)


def gelu_parts(value):
    normal_cdf = 0.5 * (1.0 + jax.scipy.special.erf(value / math.sqrt(2.0)))
    density = jnp.exp(-0.5 * value * value) / math.sqrt(2.0 * math.pi)
    return (value * normal_cdf, normal_cdf + value * density)


def with_collectives(inputs, w_conv_up, w_gate_up, w_down, taps, conv_bias, cotangent):
    span = TAPS - 1
    rows = inputs.shape[0]
    width = w_conv_up.shape[1]
    col_start = lax.axis_index("tp") * width
    taps_own = lax.dynamic_slice_in_dim(taps, col_start, width, 1)
    bias_own = lax.dynamic_slice_in_dim(conv_bias, col_start, width, 0)
    features, cot_full = (
        lax.all_gather(inputs, "tp", axis=1, tiled=True),
        lax.all_gather(cotangent, "tp", axis=1, tiled=True),
    )
    conv_weight, gate_weight = (
        lax.all_gather(w_conv_up, "fs", axis=0, tiled=True),
        lax.all_gather(w_gate_up, "fs", axis=0, tiled=True),
    )
    columns = cot_full
    d_hidden = lax.dot_general(
        columns,
        lax.all_gather(w_down, "fs", axis=1, tiled=True),
        (((1,), (1,)), ((), ())),
        preferred_element_type=jnp.float32,
    ).astype(jnp.bfloat16)
    up_a = jnp.dot(features, conv_weight, preferred_element_type=jnp.float32).astype(jnp.bfloat16)
    up_b = jnp.dot(features, gate_weight, preferred_element_type=jnp.float32).astype(jnp.bfloat16)
    earlier = shifted(up_a[rows - span :], "fs", 1)
    extended = jnp.concatenate([earlier, up_a], 0).astype(jnp.float32)
    conv_out = bias_own[None, :] + sum(
        (taps_own[i][None, :] * extended[i : i + rows] for i in range(TAPS))
    )
    gelu_value, gelu_slope = gelu_parts(conv_out)
    hidden_grad = d_hidden.astype(jnp.float32)
    d_conv = hidden_grad * up_b.astype(jnp.float32) * gelu_slope
    d_up_b = (hidden_grad * gelu_value).astype(jnp.bfloat16)
    later = shifted(d_conv[:span], "fs", -1)
    d_extended = jnp.concatenate([d_conv, later], 0)
    d_up_a = sum(
        (taps_own[i][None, :] * d_extended[span - i : span - i + rows] for i in range(TAPS))
    ).astype(jnp.bfloat16)
    tap_terms = [jnp.sum(d_conv * extended[i : i + rows], axis=0) for i in range(TAPS)]
    column_part = jnp.stack(tap_terms + [jnp.sum(d_conv, axis=0)], 0)
    contract = (((1,), (1,)), ((), ()))
    partial_sum = lax.dot_general(d_up_a, conv_weight, contract, preferred_element_type=jnp.float32)
    partial_sum = partial_sum + lax.dot_general(
        d_up_b, gate_weight, contract, preferred_element_type=jnp.float32
    )
    grad_inputs = lax.psum_scatter(
        partial_sum.astype(jnp.bfloat16), "tp", scatter_dimension=1, tiled=True
    )
    columns = features
    grad_conv_up = lax.psum_scatter(
        lax.dot_general(
            columns, d_up_a, (((0,), (0,)), ((), ())), preferred_element_type=jnp.float32
        ),
        "fs",
        scatter_dimension=0,
        tiled=True,
    )
    squares = jnp.sum(grad_conv_up * grad_conv_up, axis=0)
    placed = jnp.zeros((TAPS + 1, width * lax.axis_size("tp")), jnp.float32)
    placed = lax.dynamic_update_slice_in_dim(placed, column_part, col_start, 1)
    full_columns = lax.psum(placed, ("fs", "tp"))
    unit_norms = lax.psum(squares, "fs")
    return (grad_inputs, grad_conv_up, unit_norms, full_columns[:TAPS], full_columns[TAPS])


def greet(peers):
    barrier = pltpu.get_barrier_semaphore()
    for peer in peers:
        pl.semaphore_signal(barrier, inc=1, device_id=peer, device_id_type=MESH)
    pl.semaphore_wait(barrier, len(peers))


def dot(a, b, da, db):
    return lax.dot_general(
        a, b, (((da,), (db,)), ((), ())), preferred_element_type=jnp.float32
    )


def rounded(value):
    return value.astype(jnp.bfloat16).astype(jnp.float32)


def buffers(n, t, shard, rows, ca):
    b16, f32 = jnp.bfloat16, jnp.float32
    return dict(
        stage=pltpu.VMEM((3, shard, ca), b16),
        wbuf=pltpu.VMEM((3, n, shard, ca), b16),
        abuf=pltpu.VMEM((2, 2, n, shard, rows), b16),
        tot=pltpu.VMEM((3, 2, rows + 8, ca), f32),
        halo_up=pltpu.VMEM((2, 8, ca), f32),
        halo_dc=pltpu.VMEM((2, 8, ca), f32),
        tb=pltpu.VMEM((8, ca), f32),
        dcv=pltpu.VMEM((2, rows + 8, ca), f32),
        dup=pltpu.VMEM((2, 2, rows, ca), b16),
        col_own=pltpu.VMEM((8, ca), f32),
        col_got=pltpu.VMEM((3, 8, ca), f32),
        col_sum=pltpu.VMEM((8, ca), f32),
        col_all=pltpu.VMEM((t, 2, 8, ca), f32),
        ysend=pltpu.VMEM((4, shard, ca), b16),
        yrecv=pltpu.VMEM((4, shard, ca), b16),
        gown=pltpu.VMEM((4, shard, ca), f32),
        zsend=pltpu.VMEM((3, shard, ca), b16),
        zrecv=pltpu.VMEM((4, shard, ca), b16),
        csend=pltpu.VMEM((8, shard, rows), b16),
        crecv=pltpu.VMEM((8, shard, rows), b16),
        pown=pltpu.VMEM((8, shard, rows), f32),
        xsend=pltpu.VMEM((4, shard, rows), b16),
        xrecv=pltpu.VMEM((4, shard, rows), b16),
        psend=pltpu.VMEM((2, shard, rows), b16),
        precv=pltpu.VMEM((2, shard, rows), b16),
        norm_own=pltpu.VMEM((8, ca), f32),
        norm_all=pltpu.VMEM((n, 8, ca), f32),
    )


def semaphores(n, t):
    shapes = dict(
        wz=(3, 3), wy=(3, 4), az=(4,), ax=(2, 4), ac=(4, 4), hu=(2,), hd=(2,),
        c1=(3,), c2=(2 * t - 1,), gy=(4,), gz=(4,), pc=(8,), px=(4,), pz=(2,), nm=(n - 1,),
    )
    dma = pltpu.SemaphoreType.DMA
    return {name + end: dma(s) for name, s in shapes.items() for end in ("_s", "_r")}


def layer_kernel(n, t, names, *refs):
    w, acts, taps, bias = refs[:3], refs[3:5], refs[5], refs[6]
    i_out, g_out, norm_out, taps_out, bias_out = refs[7:12]
    m = dict(zip(names, refs[12:]))
    stage, wbuf, abuf, tot = m["stage"], m["wbuf"], m["abuf"], m["tot"]
    dcv, dup, tb = m["dcv"], m["dup"], m["tb"]
    shard, width = w[0].shape
    ca = stage.shape[2]
    cb = width - ca
    rows = acts[0].shape[2]
    me, mine = lax.axis_index("fs"), lax.axis_index("tp")
    z, y = me // 2, lax.rem(me, 2)
    x, c = mine // 2, lax.rem(mine, 2)
    l = lax.rem(z, 2)
    upper = z // 2
    zp = z + 1 - 2 * l
    zo = 3 - z
    far = 3 - zp
    inner_i = lax.rem((z + 1) // 2, 2)
    inner = inner_i == 1
    outer = inner_i == 0
    across = {"fs": z * 2 + 1 - y}
    pair = {"fs": zp * 2 + y}
    x_dev = {"tp": (1 - x) * 2 + c}
    twin = {"tp": x * 2 + 1 - c}
    x_tp = (1 - x) * 2 + c
    line = [zp, far, zo]
    started = []

    def copy(name, at, src, dst, to, slot=None):
        slot = at if slot is None else slot
        return pltpu.make_async_remote_copy(
            src_ref=src, dst_ref=dst,
            send_sem=m[name + "_s"].at[at], recv_sem=m[name + "_r"].at[slot],
            device_id=to, device_id_type=MESH,
        )

    def push(*args, **kw):
        made = copy(*args, **kw)
        made.start()
        started.append(made)
        return made

    def put(i, ref, first):
        if first:
            ref[...] = w[i][:, :ca]
        else:
            ref[:, cb // LANES * LANES :] = jnp.zeros(
                (shard, ca - cb // LANES * LANES), jnp.bfloat16
            )
            ref[:, :cb] = w[i][:, ca:]

    for i in range(3):
        for flag, first in ((inner, True), (outer, False)):
            @pl.when(flag)
            def _(i=i, first=first):
                put(i, wbuf.at[i, me], first)
                put(i, stage.at[i], not first)
    for a in range(2):
        for half in range(2):
            abuf[a, l, 2 * mine + half] = acts[a][half]
    tb[...] = jnp.zeros(tb.shape, jnp.float32)
    for p in range(t):
        for flag, start, size in ((inner, 0, ca), (outer, ca, cb)):
            @pl.when(jnp.logical_and(mine == p, flag))
            def _(p=p, start=start, size=size):
                at = p * width + start
                tb[0:3, 0:size] = taps[:, at : at + size]
                tb[3:4, 0:size] = bias[:, at : at + size]

    others = [{"fs": lax.rem(me + k, n)} for k in range(1, n)]
    others += [{"tp": lax.rem(mine + k, t)} for k in range(1, t)]
    others += [{"fs": zp * 2 + y, "tp": lax.rem(mine + k, t)} for k in range(1, t)]
    greet(others)

    quarter = [(1, 0), (1, 1), (0, 0), (0, 1)]
    own_act = [abuf.at[a, l, 2 * mine + half] for a, half in quarter]
    pair_act = [abuf.at[a, 1 - l, 2 * mine + half] for a, half in quarter]
    x_act = [abuf.at[a, l, 2 * x_tp + half] for a, half in quarter]
    xp_act = [abuf.at[a, 1 - l, 2 * x_tp + half] for a, half in quarter]
    az, ax, ac, wz, wy = {}, {}, {}, {}, {}

    def send_act(q):
        a, half = quarter[q]
        az[q] = push("az", (q,), acts[a].at[half], own_act[q], pair)
        ax[0, q] = push("ax", (0, q), acts[a].at[half], own_act[q], x_dev)
        ac[0, q] = push("ac", (0, q), acts[a].at[half], own_act[q], twin)

    def send_w(i):
        own = wbuf.at[i, me]
        for j in range(3):
            wz[i, j] = push(
                "wz", (i, j), own if j == 2 else stage.at[i], own, {"fs": line[j] * 2 + y}
            )
        wy[i, 3] = push("wy", (i, 3), own, own, across)

    def pass_w(i, j):
        wz[i, j].wait_recv()
        slot = wbuf.at[i, line[j] * 2 + y]
        wy[i, j] = push("wy", (i, j), slot, slot, across)

    def pass_pair(q):
        az[q].wait_recv()
        ax[1, q] = push("ax", (1, q), pair_act[q], pair_act[q], x_dev)
        ac[1, q] = push("ac", (1, q), pair_act[q], pair_act[q], twin)

    def pass_x(way, q):
        ax[way, q].wait_recv()
        ref = (x_act, xp_act)[way][q]
        ac[2 + way, q] = push("ac", (2 + way, q), ref, ref, twin)

    def multiply(i, zz, fresh):
        a = 1 if i == 0 else 0

        @pl.loop(0, 2)
        def _(b):
            product = dot(abuf[a, b, 2 * zz], wbuf[i, 2 * zz], 0, 0)
            product = product + dot(abuf[a, b, 2 * zz + 1], wbuf[i, 2 * zz + 1], 0, 0)
            if fresh:
                tot[i, b, 8:, :] = product
            else:
                tot[i, b, 8:, :] = tot[i, b, 8:, :] + product

    send_act(0)
    send_act(1)
    send_w(0)
    send_act(2)
    send_w(1)
    send_act(3)
    send_w(2)
    pass_pair(0)
    pass_x(0, 0)
    pass_x(0, 1)
    pass_pair(1)
    for j in range(3):
        pass_w(0, j)
    pass_x(0, 2)
    pass_x(0, 3)
    pass_x(1, 0)
    pass_pair(2)
    pass_x(1, 1)
    for j in range(3):
        pass_w(1, j)
    pass_pair(3)
    pass_x(1, 2)
    for s in range(4):
        for q in range(2):
            ac[s, q].wait_recv()
    for k, j in enumerate((3, 0, 1, 2)):
        wy[0, j].wait_recv()
        multiply(0, z if j == 3 else line[j], k == 0)
    pass_x(1, 3)
    for s in range(4):
        for q in range(2, 4):
            ac[s, q].wait_recv()
    for k, j in enumerate((3, 0, 1, 2)):
        wy[1, j].wait_recv()
        multiply(1, z if j == 3 else line[j], k == 0)
    for b in range(2):
        edge, where = tot.at[1, b, pl.ds(rows, 8)], m["halo_up"]
        if b == 0:
            hu0 = push("hu", (0,), edge, where.at[y], across, slot=(y,))
        else:
            hu_near = copy("hu", (1,), edge, where.at[1], across)
            hu_far = copy("hu", (1,), edge, where.at[0], {"fs": zo * 2}, slot=(0,))
            pl.when(y == 0)(hu_near.start)
            pl.when(jnp.logical_and(y == 1, upper == 0))(hu_far.start)
    for j in range(3):
        pass_w(2, j)

    span = 32
    steps = rows // span

    def row(k):
        return tb[k : k + 1, :]

    def gelu_rows(b, r):
        at = pl.multiple_of(r * span, span)
        around = rounded(tot[1, b, pl.ds(at, span + 8), :])
        value = row(3) + row(0) * around[6 : 6 + span]
        value = value + row(1) * around[7 : 7 + span] + row(2) * around[8 : 8 + span]
        cdf = 0.5 * (1.0 + lax.erf(value * (1.0 / math.sqrt(2.0))))
        density = jnp.exp(-0.5 * value * value) * (1.0 / math.sqrt(2.0 * math.pi))
        hidden = rounded(tot[0, b, pl.ds(at + 8, span), :])
        dup[1, b, pl.ds(at, span), :] = (hidden * (value * cdf)).astype(jnp.bfloat16)
        dcv[b, pl.ds(at, span), :] = hidden * (cdf + value * density)

    @pl.loop(0, 2 * (steps - 1))
    def _(k):
        gelu_rows(lax.rem(k, 2), 1 + k // 2)

    has_before = jnp.logical_or(y == 1, upper == 1)
    has_after = jnp.logical_or(y == 1 - 0, y == 0)
    del has_after
    wait_up = [copy("hu", (b,), m["halo_up"].at[b], m["halo_up"].at[b], across) for b in range(2)]
    wait_up[1].wait_recv()
    pl.when(has_before)(wait_up[0].wait_recv)
    tot[1, 1, 0:8, :] = m["halo_up"][1]

    @pl.when(has_before)
    def _():
        tot[1, 0, 0:8, :] = m["halo_up"][0]

    @pl.when(jnp.logical_not(has_before))
    def _():
        tot[1, 0, 0:8, :] = jnp.zeros((8, ca), jnp.float32)

    @pl.loop(0, 2)
    def _(b):
        gelu_rows(b, 0)

    for k, j in enumerate((3, 0, 1, 2)):
        wy[2, j].wait_recv()
        multiply(2, z if j == 3 else line[j], k == 0)

    def grad_rows(b, r, sums):
        at = pl.multiple_of(r * span, span)
        grad = dcv[b, pl.ds(at, span), :] * rounded(tot[2, b, pl.ds(at + 8, span), :])
        dcv[b, pl.ds(at, span), :] = grad
        around = rounded(tot[1, b, pl.ds(at, span + 8), :])

        def folded(value):
            total = value[0:8]
            for k in range(8, span, 8):
                total = total + value[k : k + 8]
            return total

        terms = [folded(grad * around[6 + i : 6 + i + span]) for i in range(3)] + [folded(grad)]
        return tuple(s + v for s, v in zip(sums, terms))

    sums = tuple(jnp.zeros((8, ca), jnp.float32) for _ in range(4))
    sums = lax.fori_loop(0, 2, lambda b, s: grad_rows(b, 0, s), sums)
    edge = dcv.at[0, pl.ds(0, 8)]
    hd_near = copy("hd", (0,), edge, m["halo_dc"].at[0], across)
    hd_far = copy("hd", (0,), edge, m["halo_dc"].at[1], {"fs": zo * 2 + 1}, slot=(1,))
    pl.when(y == 1)(hd_near.start)
    pl.when(jnp.logical_and(y == 0, upper == 1))(hd_far.start)
    push("hd", (1,), dcv.at[1, pl.ds(0, 8)], m["halo_dc"].at[y], across, slot=(y,))
    sums = lax.fori_loop(
        0, 2 * (steps - 1), lambda k, s: grad_rows(lax.rem(k, 2), 1 + k // 2, s), sums
    )
    m["col_own"][4:8, :] = jnp.zeros((4, ca), jnp.float32)
    for k in range(4):
        m["col_own"][k : k + 1, :] = jnp.sum(sums[k], axis=0, keepdims=True)
    group = [across, {"fs": zo * 2 + y}, {"fs": zo * 2 + 1 - y}]
    c1 = [push("c1", (k,), m["col_own"], m["col_got"].at[k], group[k]) for k in range(3)]

    def shift_rows(b, r):
        at = pl.multiple_of(r * span, span)
        ahead = dcv[b, pl.ds(at, span + 8), :]
        total = row(0) * ahead[2 : 2 + span] + row(1) * ahead[1 : 1 + span]
        total = total + row(2) * ahead[0:span]
        dup[0, b, pl.ds(at, span), :] = total.astype(jnp.bfloat16)

    @pl.loop(0, 2 * (steps - 1))
    def _(k):
        shift_rows(lax.rem(k, 2), k // 2)

    has_next = jnp.logical_or(y == 0, upper == 0)
    wait_dc = [copy("hd", (b,), m["halo_dc"].at[b], m["halo_dc"].at[b], across) for b in range(2)]
    wait_dc[0].wait_recv()
    pl.when(has_next)(wait_dc[1].wait_recv)
    dcv[0, rows : rows + 8, :] = m["halo_dc"][0]

    @pl.when(has_next)
    def _():
        dcv[1, rows : rows + 8, :] = m["halo_dc"][1]

    @pl.when(jnp.logical_not(has_next))
    def _():
        dcv[1, rows : rows + 8, :] = jnp.zeros((8, ca), jnp.float32)

    @pl.loop(0, 2)
    def _(b):
        shift_rows(b, steps - 1)

    def weight_grad(zz, yy):
        k = 2 * zz + yy
        return dot(abuf[0, 0, k], dup[0, 0], 1, 0) + dot(abuf[0, 1, k], dup[0, 1], 1, 0)

    def input_grad(b, k):
        return dot(wbuf[1, k], dup[0, b], 1, 1) + dot(wbuf[2, k], dup[1, b], 1, 1)

    b16, f32 = jnp.bfloat16, jnp.float32
    order = [far, zo, zp, z]
    ysend, yrecv, gown, zsend, zrecv = (m[k] for k in ("ysend", "yrecv", "gown", "zsend", "zrecv"))
    csend, crecv, pown, xsend, xrecv = (m[k] for k in ("csend", "crecv", "pown", "xsend", "xrecv"))
    psend, precv = m["psend"], m["precv"]
    gy, pc, px, pz = {}, {}, {}, {}

    def spot(bi, xi, half):
        return bi * 4 + xi * 2 + half

    def to_twin(bi, xi, half):
        b, xx, at = (1 - l, l)[bi], (1 - x, x)[xi], spot(bi, xi, half)
        csend[at] = input_grad(b, 2 * (xx * 2 + 1 - c) + half).astype(b16)
        pc[at] = push("pc", (at,), csend.at[at], crecv.at[at], twin)

    def keep(bi, xi, half):
        b, xx, at = (1 - l, l)[bi], (1 - x, x)[xi], spot(bi, xi, half)
        pown[at] = input_grad(b, 2 * (xx * 2 + c) + half)

    def to_x(bi, half):
        at, to = spot(bi, 0, half), bi * 2 + half
        pc[at].wait_recv()
        xsend[to] = (pown[at] + crecv[at].astype(f32)).astype(b16)
        px[to] = push("px", (to,), xsend.at[to], xrecv.at[to], x_dev)

    def to_pair(half):
        at = spot(0, 1, half)
        pc[at].wait_recv()
        px[half].wait_recv()
        total = pown[at] + crecv[at].astype(f32) + xrecv[half].astype(f32)
        psend[half] = total.astype(b16)
        pz[half] = push("pz", (half,), psend.at[half], precv.at[half], pair)

    def finish(half):
        at = spot(1, 1, half)
        pc[at].wait_recv()
        px[2 + half].wait_recv()
        pz[half].wait_recv()
        total = pown[at] + crecv[at].astype(f32)
        total = total + xrecv[2 + half].astype(f32) + precv[half].astype(f32)
        i_out[half] = total.astype(b16)

    for k in range(4):
        ysend[k] = weight_grad(order[k], 1 - y).astype(b16)
        gy[k] = push("gy", (k,), ysend.at[k], yrecv.at[k], across)
    for bi in range(2):
        for half in range(2):
            to_twin(bi, 0, half)
        for half in range(2):
            keep(bi, 0, half)
            to_x(bi, half)
    for k in range(4):
        gown[k] = weight_grad(order[k], y)

    def summed(k):
        gy[k].wait_recv()
        return gown[k] + yrecv[k].astype(f32)

    for k in range(3):
        c1[k].wait_recv()
    got = m["col_got"]
    m["col_sum"][...] = (m["col_own"][...] + got[0]) + (got[1] + got[2])
    place = m["col_all"].at[mine, 1 - inner_i]
    place[...] = m["col_sum"][...]
    c2 = []
    for k in range(1, 2 * t):
        tp = lax.rem(mine + k // 2, t)
        to = {"fs": (zp if k % 2 else z) * 2 + y, "tp": tp}
        c2.append(push("c2", (k - 1,), m["col_sum"], place, to))

    gz_wait = [copy("gz", (k,), zrecv.at[k], zrecv.at[k], across) for k in range(4)]
    zsend[0] = summed(0).astype(b16)
    first_to = inner_i * zo + (1 - inner_i) * far
    first_at = 3 - 2 * inner_i
    push("gz", (0,), zsend.at[0], zrecv.at[first_at], {"fs": first_to * 2 + y}, slot=(first_at,))
    zsend[1] = summed(1).astype(b16)
    push("gz", (1,), zsend.at[1], zrecv.at[0], {"fs": zo * 2 + y}, slot=(0,))
    for bi in range(2):
        for half in range(2):
            to_twin(bi, 1, half)
        for half in range(2):
            keep(bi, 1, half)
    to_pair(0)
    gown[2] = summed(2)

    @pl.when(outer)
    def _():
        zsend[2] = gown[2].astype(b16)

    @pl.when(inner)
    def _():
        gz_wait[1].wait_recv()
        zsend[2] = (gown[2] + zrecv[1].astype(f32)).astype(b16)

    last_at = 1 + (1 - inner_i)
    push("gz", (2,), zsend.at[2], zrecv.at[last_at], pair, slot=(last_at,))
    to_pair(1)
    gown[3] = summed(3)
    gz_wait[0].wait_recv()
    norm_own, norm_all = m["norm_own"], m["norm_all"]
    norm_own[...] = jnp.zeros(norm_own.shape, f32)

    def settle(k, value):
        g_out[:, k * ca : k * ca + (cb if k else ca)] = value[:, : (cb if k else ca)]
        norm_own[k : k + 1, :] = jnp.sum(value * value, axis=0, keepdims=True)

    @pl.when(inner)
    def _():
        settle(0, gown[3] + zrecv[0].astype(f32))
        gz_wait[2].wait_recv()
        gz_wait[3].wait_recv()
        settle(1, zrecv[2].astype(f32) + zrecv[3].astype(f32))

    @pl.when(outer)
    def _():
        settle(1, gown[3] + zrecv[0].astype(f32))
        gz_wait[1].wait_recv()
        settle(0, zrecv[1].astype(f32))

    norms = [
        push("nm", (k,), norm_own, norm_all.at[me], others[k]) for k in range(n - 1)
    ]
    finish(0)
    for copy_in in c2:
        copy_in.wait_recv()
    whole = m["col_all"]
    for p in range(t):
        at = p * width
        taps_out[:, at : at + ca] = whole[p, 0, 0:3, :]
        taps_out[:, at + ca : at + width] = whole[p, 1, 0:3, :cb]
        bias_out[:, at : at + ca] = whole[p, 0, 3:4, :]
        bias_out[:, at + ca : at + width] = whole[p, 1, 3:4, :cb]
    finish(1)
    for copy_in in norms:
        copy_in.wait_recv()
    norm_all[me] = norm_own[...]
    total = norm_all[0]
    for k in range(1, n):
        total = total + norm_all[k]
    norm_out[:, :ca] = total[0:1, :]
    norm_out[:, ca:] = total[1:2, :cb]
    for made in started:
        made.wait_send()
    pl.when(y == 0)(hu_near.wait_send)
    pl.when(jnp.logical_and(y == 1, upper == 0))(hu_far.wait_send)
    pl.when(y == 1)(hd_near.wait_send)
    pl.when(jnp.logical_and(y == 0, upper == 1))(hd_far.wait_send)


def with_kernel(inputs, w_conv_up, w_gate_up, w_down, taps, conv_bias, cotangent):
    n, t = lax.axis_size("fs"), lax.axis_size("tp")
    rows = inputs.shape[0]
    shard, width = w_conv_up.shape
    ca = -(-width // (2 * LANES)) * LANES
    shape = jax.ShapeDtypeStruct
    scratch = {**buffers(n, t, shard, rows, ca), **semaphores(n, t)}
    acts = [v.T.reshape(2, shard, rows) for v in (inputs, cotangent)]
    got = pl.pallas_call(
        functools.partial(layer_kernel, n, t, tuple(scratch)),
        out_shape=[
            shape((2, shard, rows), jnp.bfloat16),
            shape((shard, width), jnp.float32),
            shape((1, width), jnp.float32),
            shape((TAPS, t * width), jnp.float32),
            shape((1, t * width), jnp.float32),
        ],
        in_specs=[VMEM] * 7,
        out_specs=[VMEM] * 5,
        scratch_shapes=list(scratch.values()),
        compiler_params=pltpu.CompilerParams(
            collective_id=0, has_side_effects=True, vmem_limit_bytes=60 * 1024 * 1024
        ),
        name="layer",
    )(w_down.T, w_conv_up, w_gate_up, *acts, taps, conv_bias[None, :])
    grad_inputs, grad_conv_up, norms, grad_taps, grad_bias = got
    return (grad_inputs.reshape(-1, rows).T, grad_conv_up, norms[0], grad_taps, grad_bias[0])


def per_device(inputs, w_conv_up, *rest):
    n, t = lax.axis_size("fs"), lax.axis_size("tp")
    shard, width = w_conv_up.shape
    rows, features = inputs.shape
    fits = n == 8 and t == 4 and features == 2 * shard
    aligned = shard % 8 == 0 and rows % LANES == 0 and width > LANES
    chosen = with_kernel if fits and aligned else with_collectives
    return chosen(inputs, w_conv_up, *rest)


def solution(mesh):
    return jax.shard_map(
        per_device,
        mesh=mesh,
        in_specs=(
            P("fs", "tp"),
            P("fs", "tp"),
            P("fs", "tp"),
            P("tp", "fs"),
            P(),
            P(),
            P("fs", "tp"),
        ),
        out_specs=(P("fs", "tp"), P("fs", "tp"), P("tp"), P(), P()),
        check_vma=False,
    )
```

```python
import functools
import math

import jax
import jax.numpy as jnp
from jax import lax
from jax.experimental import pallas as pl
from jax.experimental.pallas import tpu as pltpu
from jax.sharding import PartitionSpec as P

TAPS = 3
LANES = 128
MESH = pl.DeviceIdType.MESH
VMEM_BYTES = 63 * 1024 * 1024
ANY = pl.BlockSpec(memory_space=pl.ANY)


def shifted(block, axis, distance):
    devices = range(lax.axis_size(axis))
    route = [(i - distance, i) for i in devices if i - distance in devices]
    return lax.ppermute(block, axis, route)


def gelu_parts(value):
    normal_cdf = 0.5 * (1.0 + jax.scipy.special.erf(value / math.sqrt(2.0)))
    density = jnp.exp(-0.5 * value * value) / math.sqrt(2.0 * math.pi)
    return (value * normal_cdf, normal_cdf + value * density)


def with_collectives(inputs, w_conv_up, w_gate_up, w_down, taps, conv_bias, cotangent):
    span = TAPS - 1
    rows = inputs.shape[0]
    width = w_conv_up.shape[1]
    col_start = lax.axis_index("tp") * width
    taps_own = lax.dynamic_slice_in_dim(taps, col_start, width, 1)
    bias_own = lax.dynamic_slice_in_dim(conv_bias, col_start, width, 0)
    features, cot_full = (
        lax.all_gather(inputs, "tp", axis=1, tiled=True),
        lax.all_gather(cotangent, "tp", axis=1, tiled=True),
    )
    conv_weight, gate_weight = (
        lax.all_gather(w_conv_up, "fs", axis=0, tiled=True),
        lax.all_gather(w_gate_up, "fs", axis=0, tiled=True),
    )
    columns = cot_full
    d_hidden = lax.dot_general(
        columns,
        lax.all_gather(w_down, "fs", axis=1, tiled=True),
        (((1,), (1,)), ((), ())),
        preferred_element_type=jnp.float32,
    ).astype(jnp.bfloat16)
    up_a = jnp.dot(features, conv_weight, preferred_element_type=jnp.float32).astype(jnp.bfloat16)
    up_b = jnp.dot(features, gate_weight, preferred_element_type=jnp.float32).astype(jnp.bfloat16)
    earlier = shifted(up_a[rows - span :], "fs", 1)
    extended = jnp.concatenate([earlier, up_a], 0).astype(jnp.float32)
    conv_out = bias_own[None, :] + sum(
        (taps_own[i][None, :] * extended[i : i + rows] for i in range(TAPS))
    )
    gelu_value, gelu_slope = gelu_parts(conv_out)
    hidden_grad = d_hidden.astype(jnp.float32)
    d_conv = hidden_grad * up_b.astype(jnp.float32) * gelu_slope
    d_up_b = (hidden_grad * gelu_value).astype(jnp.bfloat16)
    later = shifted(d_conv[:span], "fs", -1)
    d_extended = jnp.concatenate([d_conv, later], 0)
    d_up_a = sum(
        (taps_own[i][None, :] * d_extended[span - i : span - i + rows] for i in range(TAPS))
    ).astype(jnp.bfloat16)
    tap_terms = [jnp.sum(d_conv * extended[i : i + rows], axis=0) for i in range(TAPS)]
    column_part = jnp.stack(tap_terms + [jnp.sum(d_conv, axis=0)], 0)
    contract = (((1,), (1,)), ((), ()))
    partial_sum = lax.dot_general(d_up_a, conv_weight, contract, preferred_element_type=jnp.float32)
    partial_sum = partial_sum + lax.dot_general(
        d_up_b, gate_weight, contract, preferred_element_type=jnp.float32
    )
    grad_inputs = lax.psum_scatter(
        partial_sum.astype(jnp.bfloat16), "tp", scatter_dimension=1, tiled=True
    )
    columns = features
    grad_conv_up = lax.psum_scatter(
        lax.dot_general(
            columns, d_up_a, (((0,), (0,)), ((), ())), preferred_element_type=jnp.float32
        ),
        "fs",
        scatter_dimension=0,
        tiled=True,
    )
    squares = jnp.sum(grad_conv_up * grad_conv_up, axis=0)
    placed = jnp.zeros((TAPS + 1, width * lax.axis_size("tp")), jnp.float32)
    placed = lax.dynamic_update_slice_in_dim(placed, column_part, col_start, 1)
    full_columns = lax.psum(placed, ("fs", "tp"))
    unit_norms = lax.psum(squares, "fs")
    return (grad_inputs, grad_conv_up, unit_norms, full_columns[:TAPS], full_columns[TAPS])


def greet(peers):
    barrier = pltpu.get_barrier_semaphore()
    for peer in peers:
        pl.semaphore_signal(barrier, inc=1, device_id=peer, device_id_type=MESH)


def greeted(peers):
    pl.semaphore_wait(pltpu.get_barrier_semaphore(), len(peers))


def dot(a, b, da, db):
    return lax.dot_general(
        a, b, (((da,), (db,)), ((), ())), preferred_element_type=jnp.float32
    )


def rounded(value):
    return value.astype(jnp.bfloat16).astype(jnp.float32)


def buffers(n, t, shard, width, rows, ca):
    b16, f32 = jnp.bfloat16, jnp.float32
    return dict(
        wv=pltpu.VMEM((3, shard, width), b16),
        taps_v=pltpu.VMEM((TAPS, t * width), f32),
        bias_v=pltpu.VMEM((t * width,), f32),
        i_v=pltpu.VMEM((2, shard, rows), b16),
        g_v=pltpu.VMEM((shard, width), f32),
        norm_v=pltpu.VMEM((width,), f32),
        taps_w=pltpu.VMEM((TAPS, t * width), f32),
        bias_w=pltpu.VMEM((t * width,), f32),
        stage=pltpu.VMEM((2, 3, shard, ca), b16),
        wbuf=pltpu.VMEM((3, n, shard, ca), b16),
        abuf=pltpu.VMEM((2, 2, n, shard, rows), b16),
        tot=pltpu.VMEM((3, 2, rows + 8, ca), f32),
        halo_up=pltpu.VMEM((2, 8, ca), f32),
        halo_dc=pltpu.VMEM((2, 8, ca), f32),
        tb=pltpu.VMEM((8, ca), f32),
        dcv=pltpu.VMEM((2, rows + 8, ca), f32),
        dup=pltpu.VMEM((2, 2, rows, ca), b16),
        col_own=pltpu.VMEM((8, ca), f32),
        col_got=pltpu.VMEM((3, 8, ca), f32),
        col_sum=pltpu.VMEM((8, ca), f32),
        col_all=pltpu.VMEM((t, 2, 8, ca), f32),
        ysend=pltpu.VMEM((4, shard, ca), b16),
        yrecv=pltpu.VMEM((4, shard, ca), b16),
        gown=pltpu.VMEM((4, shard, ca), f32),
        zsend=pltpu.VMEM((3, shard, ca), b16),
        zrecv=pltpu.VMEM((4, shard, ca), b16),
        csend=pltpu.VMEM((8, shard, rows), b16),
        crecv=pltpu.VMEM((8, shard, rows), b16),
        pown=pltpu.VMEM((8, shard, rows), f32),
        xsend=pltpu.VMEM((4, shard, rows), b16),
        xrecv=pltpu.VMEM((4, shard, rows), b16),
        psend=pltpu.VMEM((2, shard, rows), b16),
        precv=pltpu.VMEM((2, shard, rows), b16),
        norm_own=pltpu.VMEM((8, ca), f32),
        norm_all=pltpu.VMEM((n, 8, ca), f32),
    )


def semaphores(n, t):
    shapes = dict(
        wz=(3, 3), wy=(3, 4), az=(4,), ax=(2, 4), ac=(4, 4), hu=(2,), hd=(2,),
        c1=(3,), c2=(2 * t - 1,), gy=(4, 2), gz=(4, 2), pc=(8,), px=(4,), pz=(2,), nm=(n - 1,),
    )
    dma = pltpu.SemaphoreType.DMA
    local = dict(ld=dma((9,)), st=dma((6,)))
    return local | {name + end: dma(s) for name, s in shapes.items() for end in ("_s", "_r")}


def layer_kernel(n, t, names, *refs):
    w_in, acts, taps_in, bias_in = refs[:3], refs[3:5], refs[5], refs[6]
    outs = refs[7:12]
    m = dict(zip(names, refs[12:]))
    stage, wbuf, abuf, tot = m["stage"], m["wbuf"], m["abuf"], m["tot"]
    dcv, dup, tb = m["dcv"], m["dup"], m["tb"]
    w, taps, bias = m["wv"], m["taps_v"], m["bias_v"]
    shard, width = w.shape[1:]
    ca = stage.shape[3]
    cb = width - ca
    rows = acts[0].shape[2]
    me, mine = lax.axis_index("fs"), lax.axis_index("tp")
    z, y = me // 2, lax.rem(me, 2)
    x, c = mine // 2, lax.rem(mine, 2)
    l = lax.rem(z, 2)
    upper = z // 2
    zp = z + 1 - 2 * l
    zo = 3 - z
    far = 3 - zp
    inner_i = lax.rem((z + 1) // 2, 2)
    inner = inner_i == 1
    outer = inner_i == 0
    across = {"fs": z * 2 + 1 - y}
    pair = {"fs": zp * 2 + y}
    x_dev = {"tp": (1 - x) * 2 + c}
    twin = {"tp": x * 2 + 1 - c}
    x_tp = (1 - x) * 2 + c
    line = [zp, 2 - upper, 3 * (1 - upper)]
    started = []

    def copy(name, at, src, dst, to, slot=None):
        slot = at if slot is None else slot
        return pltpu.make_async_remote_copy(
            src_ref=src, dst_ref=dst,
            send_sem=m[name + "_s"].at[at], recv_sem=m[name + "_r"].at[slot],
            device_id=to, device_id_type=MESH,
        )

    def push(*args, **kw):
        made = copy(*args, **kw)
        made.start()
        started.append(made)
        return made

    def put(i, ref, first):
        if first:
            ref[...] = w[i, :, :ca]
        else:
            ref[:, cb // LANES * LANES :] = jnp.zeros(
                (shard, ca - cb // LANES * LANES), jnp.bfloat16
            )
            ref[:, :cb] = w[i, :, ca:]

    others = [{"fs": lax.rem(me + k, n)} for k in range(1, n)]
    others += [{"tp": lax.rem(mine + k, t)} for k in range(1, t)]
    others += [{"fs": zp * 2 + y, "tp": lax.rem(mine + k, t)} for k in range(1, t)]
    greet(others)
    loads = []

    def load(src, dst):
        made = pltpu.make_async_copy(src, dst, m["ld"].at[len(loads)])
        made.start()
        loads.append(made)

    for i in range(3):
        load(w_in[i], w.at[i])
    for a in range(2):
        for half in range(2):
            load(acts[a].at[half], abuf.at[a, l, 2 * mine + half])
    load(taps_in, taps)
    load(bias_in, bias)
    for i in range(3):
        loads[i].wait()
        put(i, stage.at[0, i], True)
        put(i, stage.at[1, i], False)
        wbuf[i, me] = stage[1 - inner_i, i]
    for made in loads[3:]:
        made.wait()
    tb[...] = jnp.zeros(tb.shape, jnp.float32)
    for p in range(t):
        for flag, start, size in ((inner, 0, ca), (outer, ca, cb)):
            @pl.when(jnp.logical_and(mine == p, flag))
            def _(p=p, start=start, size=size):
                at = p * width + start
                tb[0:3, 0:size] = taps[:, at : at + size]
                tb[3:4, 0:size] = bias[at : at + size].reshape(1, size)

    greeted(others)

    quarter = [(1, 0), (1, 1), (0, 0), (0, 1)]
    own_act = [abuf.at[a, l, 2 * mine + half] for a, half in quarter]
    pair_act = [abuf.at[a, 1 - l, 2 * mine + half] for a, half in quarter]
    x_act = [abuf.at[a, l, 2 * x_tp + half] for a, half in quarter]
    xp_act = [abuf.at[a, 1 - l, 2 * x_tp + half] for a, half in quarter]
    az, ax, ac, wz, wy = {}, {}, {}, {}, {}

    def send_act(q):
        az[q] = push("az", (q,), own_act[q], own_act[q], pair)
        ax[0, q] = push("ax", (0, q), own_act[q], own_act[q], x_dev)
        ac[0, q] = push("ac", (0, q), own_act[q], own_act[q], twin)

    def send_w(i, j):
        own = wbuf.at[i, me]
        if j == 3:
            wy[i, 3] = push("wy", (i, 3), own, own, across)
        else:
            src = stage.at[inner_i if j == 0 else j - 1, i]
            label = 0 if j == 0 else 2 - inner_i
            push("wz", (i, j), src, own, {"fs": line[j] * 2 + y}, slot=(i, label))

    def pass_w(i, j):
        slot = wbuf.at[i, line[j] * 2 + y]
        copy("wz", (i, j), slot, slot, pair).wait_recv()
        wy[i, j] = push("wy", (i, j), slot, slot, across)

    def pass_pair(q):
        az[q].wait_recv()
        ax[1, q] = push("ax", (1, q), pair_act[q], pair_act[q], x_dev)
        ac[1, q] = push("ac", (1, q), pair_act[q], pair_act[q], twin)

    def pass_x(way, q):
        ax[way, q].wait_recv()
        ref = (x_act, xp_act)[way][q]
        ac[2 + way, q] = push("ac", (2 + way, q), ref, ref, twin)

    def multiply(i, zz, b, fresh):
        a = 1 if i == 0 else 0
        product = dot(abuf[a, b, 2 * zz], wbuf[i, 2 * zz], 0, 0)
        product = product + dot(abuf[a, b, 2 * zz + 1], wbuf[i, 2 * zz + 1], 0, 0)
        if fresh:
            tot[i, b, 8:, :] = product
        else:
            tot[i, b, 8:, :] = tot[i, b, 8:, :] + product

    arrived, acts_seen = set(), set()

    def compute(i, j, which):
        if (i, j) not in arrived:
            arrived.add((i, j))
            wy[i, j].wait_recv()
        for q in (0, 1) if i == 0 else (2, 3):
            for s in (0, 2) if which == 0 else (1, 3):
                if (s, q) not in acts_seen:
                    acts_seen.add((s, q))
                    ac[s, q].wait_recv()
        multiply(i, z if j == 3 else line[j], l if which == 0 else 1 - l, j == 3)

    sending = (
        "a0 a1 w03 w02", "w01 w13 a2 w00", "w12 w11 w23 a3", "w22 w21 w10 w20",
    )
    for item in " ".join(sending).split():
        if item[0] == "a":
            send_act(int(item[1]))
        else:
            send_w(int(item[1]), int(item[2]))
    passing = (
        "x00 w01 p0", "x01 c030 x02 w02", "p1 c010 x03 w11", "c130 c230 x10 p2",
        "c020 w12 x11 c110", "c031 w00 c011 w21", "x12 c120 c021 p3", "w22 c000 c001 w10",
        "c210 x13 c220 c131", "c111 w20 c121 c100", "c101",
    )
    for item in " ".join(passing).split():
        at = [int(v) for v in item[1:]]
        dict(x=pass_x, w=pass_w, p=pass_pair, c=compute)[item[0]](*at)
    for b in range(2):
        edge, where = tot.at[1, b, pl.ds(rows, 8)], m["halo_up"]
        if b == 0:
            push("hu", (0,), edge, where.at[y], across, slot=(y,))
        else:
            hu_near = copy("hu", (1,), edge, where.at[1], across)
            hu_far = copy("hu", (1,), edge, where.at[0], {"fs": zo * 2}, slot=(0,))
            pl.when(y == 0)(hu_near.start)
            pl.when(jnp.logical_and(y == 1, upper == 0))(hu_far.start)

    span = 32
    steps = rows // span

    def row(k):
        return tb[k : k + 1, :]

    def gelu_rows(b, r):
        at = pl.multiple_of(r * span, span)
        around = rounded(tot[1, b, pl.ds(at, span + 8), :])
        value = row(3) + row(0) * around[6 : 6 + span]
        value = value + row(1) * around[7 : 7 + span] + row(2) * around[8 : 8 + span]
        cdf = 0.5 * (1.0 + lax.erf(value * (1.0 / math.sqrt(2.0))))
        density = jnp.exp(-0.5 * value * value) * (1.0 / math.sqrt(2.0 * math.pi))
        hidden = rounded(tot[0, b, pl.ds(at + 8, span), :])
        dup[1, b, pl.ds(at, span), :] = (hidden * (value * cdf)).astype(jnp.bfloat16)
        dcv[b, pl.ds(at, span), :] = hidden * (cdf + value * density)

    @pl.loop(0, 2 * (steps - 1))
    def _(k):
        gelu_rows(lax.rem(k, 2), 1 + k // 2)

    for j in (3, 1, 2):
        compute(2, j, 1)
    has_before = jnp.logical_or(y == 1, upper == 1)
    wait_up = [copy("hu", (b,), m["halo_up"].at[b], m["halo_up"].at[b], across) for b in range(2)]
    wait_up[1].wait_recv()
    pl.when(has_before)(wait_up[0].wait_recv)
    tot[1, 1, 0:8, :] = m["halo_up"][1]

    @pl.when(has_before)
    def _():
        tot[1, 0, 0:8, :] = m["halo_up"][0]

    @pl.when(jnp.logical_not(has_before))
    def _():
        tot[1, 0, 0:8, :] = jnp.zeros((8, ca), jnp.float32)

    @pl.loop(0, 2)
    def _(b):
        gelu_rows(b, 0)

    for which in range(2):
        compute(2, 0, which)

    def grad_rows(b, r, sums):
        at = pl.multiple_of(r * span, span)
        grad = dcv[b, pl.ds(at, span), :] * rounded(tot[2, b, pl.ds(at + 8, span), :])
        dcv[b, pl.ds(at, span), :] = grad
        around = rounded(tot[1, b, pl.ds(at, span + 8), :])

        def folded(value):
            total = value[0:8]
            for k in range(8, span, 8):
                total = total + value[k : k + 8]
            return total

        terms = [folded(grad * around[6 + i : 6 + i + span]) for i in range(3)] + [folded(grad)]
        return tuple(s + v for s, v in zip(sums, terms))

    sums = tuple(jnp.zeros((8, ca), jnp.float32) for _ in range(4))
    sums = lax.fori_loop(0, 2, lambda b, s: grad_rows(b, 0, s), sums)
    edge = dcv.at[0, pl.ds(0, 8)]
    hd_near = copy("hd", (0,), edge, m["halo_dc"].at[0], across)
    hd_far = copy("hd", (0,), edge, m["halo_dc"].at[1], {"fs": zo * 2 + 1}, slot=(1,))
    pl.when(y == 1)(hd_near.start)
    pl.when(jnp.logical_and(y == 0, upper == 1))(hd_far.start)
    push("hd", (1,), dcv.at[1, pl.ds(0, 8)], m["halo_dc"].at[y], across, slot=(y,))
    sums = lax.fori_loop(
        0, 2 * (steps - 1), lambda k, s: grad_rows(lax.rem(k, 2), 1 + k // 2, s), sums
    )
    m["col_own"][4:8, :] = jnp.zeros((4, ca), jnp.float32)
    for k in range(4):
        m["col_own"][k : k + 1, :] = jnp.sum(sums[k], axis=0, keepdims=True)
    group = [across, {"fs": zo * 2 + y}, {"fs": zo * 2 + 1 - y}]
    c1 = [push("c1", (k,), m["col_own"], m["col_got"].at[k], group[k]) for k in range(3)]

    def shift_rows(b, r):
        at = pl.multiple_of(r * span, span)
        ahead = dcv[b, pl.ds(at, span + 8), :]
        total = row(0) * ahead[2 : 2 + span] + row(1) * ahead[1 : 1 + span]
        total = total + row(2) * ahead[0:span]
        dup[0, b, pl.ds(at, span), :] = total.astype(jnp.bfloat16)

    @pl.loop(0, 2 * (steps - 1))
    def _(k):
        shift_rows(lax.rem(k, 2), k // 2)

    has_next = jnp.logical_or(y == 0, upper == 0)
    wait_dc = [copy("hd", (b,), m["halo_dc"].at[b], m["halo_dc"].at[b], across) for b in range(2)]
    wait_dc[0].wait_recv()
    pl.when(has_next)(wait_dc[1].wait_recv)
    dcv[0, rows : rows + 8, :] = m["halo_dc"][0]

    @pl.when(has_next)
    def _():
        dcv[1, rows : rows + 8, :] = m["halo_dc"][1]

    @pl.when(jnp.logical_not(has_next))
    def _():
        dcv[1, rows : rows + 8, :] = jnp.zeros((8, ca), jnp.float32)

    @pl.loop(0, 2)
    def _(b):
        shift_rows(b, steps - 1)

    def weight_grad(zz, yy):
        k = 2 * zz + yy
        return dot(abuf[0, 0, k], dup[0, 0], 1, 0) + dot(abuf[0, 1, k], dup[0, 1], 1, 0)

    def input_grad(b, k):
        return dot(wbuf[1, k], dup[0, b], 1, 1) + dot(wbuf[2, k], dup[1, b], 1, 1)

    b16, f32 = jnp.bfloat16, jnp.float32
    order = [far, zo, zp, z]
    ysend, yrecv, gown, zsend, zrecv = (m[k] for k in ("ysend", "yrecv", "gown", "zsend", "zrecv"))
    csend, crecv, pown, xsend, xrecv = (m[k] for k in ("csend", "crecv", "pown", "xsend", "xrecv"))
    psend, precv = m["psend"], m["precv"]
    gy, pc, px, pz = {}, {}, {}, {}

    def spot(bi, xi, half):
        return bi * 4 + xi * 2 + half

    def to_twin(bi, xi, half):
        b, xx, at = (1 - l, l)[bi], (1 - x, x)[xi], spot(bi, xi, half)
        csend[at] = input_grad(b, 2 * (xx * 2 + 1 - c) + half).astype(b16)
        pc[at] = push("pc", (at,), csend.at[at], crecv.at[at], twin)

    def keep(bi, xi, half):
        b, xx, at = (1 - l, l)[bi], (1 - x, x)[xi], spot(bi, xi, half)
        pown[at] = input_grad(b, 2 * (xx * 2 + c) + half)

    def to_x(bi, half):
        at, to = spot(bi, 0, half), bi * 2 + half
        pc[at].wait_recv()
        xsend[to] = (pown[at] + crecv[at].astype(f32)).astype(b16)
        px[to] = push("px", (to,), xsend.at[to], xrecv.at[to], x_dev)

    def to_pair(half):
        at = spot(0, 1, half)
        pc[at].wait_recv()
        px[half].wait_recv()
        total = pown[at] + crecv[at].astype(f32) + xrecv[half].astype(f32)
        psend[half] = total.astype(b16)
        pz[half] = push("pz", (half,), psend.at[half], precv.at[half], pair)

    i_v, g_v, norm_v, taps_w, bias_w = (
        m[k] for k in ("i_v", "g_v", "norm_v", "taps_w", "bias_w")
    )
    stores = []

    def store(src, dst):
        made = pltpu.make_async_copy(src, dst, m["st"].at[len(stores)])
        made.start()
        stores.append(made)

    def finish(half):
        at = spot(1, 1, half)
        pc[at].wait_recv()
        px[2 + half].wait_recv()
        pz[half].wait_recv()
        total = pown[at] + crecv[at].astype(f32)
        total = total + xrecv[2 + half].astype(f32) + precv[half].astype(f32)
        i_v[half] = total.astype(b16)
        store(i_v.at[half], outs[0].at[half])

    first_rows = -(-shard // 16) * 8
    parts = (pl.ds(0, first_rows), pl.ds(first_rows, shard - first_rows))
    first_to = inner_i * zo + (1 - inner_i) * far
    first_at = 3 - 2 * inner_i
    last_at = 2 - inner_i

    def to_across(k):
        ysend[k] = weight_grad(order[k], 1 - y).astype(b16)
        for s, at in enumerate(parts):
            gy[k, s] = push("gy", (k, s), ysend.at[k, at], yrecv.at[k, at], across)

    def own(k):
        gown[k] = weight_grad(order[k], y)

    def add_across(k, s):
        gy[k, s].wait_recv()
        at = parts[s]
        gown[k, at, :] = gown[k, at, :] + yrecv[k, at, :].astype(f32)

    def to_line(k, s, dev, slot):
        at = parts[s]
        push(
            "gz", (k, s), zsend.at[k, at], zrecv.at[slot, at], {"fs": dev * 2 + y}, slot=(slot, s)
        )

    def got_line(k, s):
        at = parts[s]
        copy("gz", (k, s), zrecv.at[k, at], zrecv.at[k, at], across).wait_recv()

    def send_columns():
        for k in range(3):
            c1[k].wait_recv()
        got = m["col_got"]
        m["col_sum"][...] = (m["col_own"][...] + got[0]) + (got[1] + got[2])
        place = m["col_all"].at[mine, 1 - inner_i]
        place[...] = m["col_sum"][...]
        for k in range(1, 2 * t):
            tp = lax.rem(mine + k // 2, t)
            to = {"fs": (zp if k % 2 else z) * 2 + y, "tp": tp}
            c2.append(push("c2", (k - 1,), m["col_sum"], place, to))

    c2 = []
    to_across(0)
    to_twin(0, 0, 0)
    to_across(1)
    to_twin(0, 0, 1)
    keep(0, 0, 0)
    send_columns()
    to_x(0, 0)
    keep(0, 0, 1)
    to_x(0, 1)
    to_across(2)
    to_across(3)
    own(0)
    for s in range(2):
        add_across(0, s)
        zsend[0, parts[s], :] = gown[0, parts[s], :].astype(b16)
        to_line(0, s, first_to, first_at)
    own(1)
    to_twin(1, 0, 0)
    to_twin(1, 0, 1)
    keep(1, 0, 0)
    to_x(1, 0)
    for s in range(2):
        add_across(1, s)
        zsend[1, parts[s], :] = gown[1, parts[s], :].astype(b16)
        to_line(1, s, zo, 0)
    keep(1, 0, 1)
    to_x(1, 1)
    own(2)
    to_twin(0, 1, 0)
    to_twin(0, 1, 1)
    keep(0, 1, 0)
    keep(0, 1, 1)
    for s in range(2):
        add_across(2, s)

        @pl.when(outer)
        def _(at=parts[s]):
            zsend[2, at, :] = gown[2, at, :].astype(b16)

        @pl.when(inner)
        def _(s=s, at=parts[s]):
            got_line(1, s)
            zsend[2, at, :] = (gown[2, at, :] + zrecv[1, at, :].astype(f32)).astype(b16)

        to_line(2, s, zp, last_at)
    to_pair(0)
    own(3)
    for half in range(2):
        to_twin(1, 1, half)
        keep(1, 1, half)
    for s in range(2):
        add_across(3, s)
        got_line(0, s)
    norm_own, norm_all = m["norm_own"], m["norm_all"]
    norm_own[...] = jnp.zeros(norm_own.shape, f32)

    def settle(k, value):
        g_v[:, k * ca : k * ca + (cb if k else ca)] = value[:, : (cb if k else ca)]
        norm_own[k : k + 1, :] = jnp.sum(value * value, axis=0, keepdims=True)

    @pl.when(inner)
    def _():
        settle(0, gown[3] + zrecv[0].astype(f32))
        for s in range(2):
            got_line(2, s)
            got_line(3, s)
        settle(1, zrecv[2].astype(f32) + zrecv[3].astype(f32))

    @pl.when(outer)
    def _():
        settle(1, gown[3] + zrecv[0].astype(f32))
        for s in range(2):
            got_line(1, s)
        settle(0, zrecv[1].astype(f32))

    norms = [
        push("nm", (k,), norm_own, norm_all.at[me], others[k]) for k in range(n - 1)
    ]
    to_pair(1)
    store(g_v, outs[1])
    finish(0)
    for copy_in in c2:
        copy_in.wait_recv()
    whole = m["col_all"]
    for p in range(t):
        at = p * width
        taps_w[:, at : at + ca] = whole[p, 0, 0:3, :]
        taps_w[:, at + ca : at + width] = whole[p, 1, 0:3, :cb]
        bias_w[at : at + ca] = whole[p, 0, 3, :]
        bias_w[at + ca : at + width] = whole[p, 1, 3, :cb]
    store(taps_w, outs[3])
    store(bias_w, outs[4])
    finish(1)
    for copy_in in norms:
        copy_in.wait_recv()
    norm_all[me] = norm_own[...]
    total = norm_all[0]
    for k in range(1, n):
        total = total + norm_all[k]
    norm_v[:ca] = total[0]
    norm_v[ca:] = total[1, :cb]
    store(norm_v, outs[2])
    for made in started:
        made.wait_send()
    for made in stores:
        made.wait()
    pl.when(y == 0)(hu_near.wait_send)
    pl.when(jnp.logical_and(y == 1, upper == 0))(hu_far.wait_send)
    pl.when(y == 1)(hd_near.wait_send)
    pl.when(jnp.logical_and(y == 0, upper == 1))(hd_far.wait_send)


def publish_kernel(n, *refs):
    src, dst, held, sem = refs[:n], refs[n : 2 * n], refs[2 * n : 3 * n], refs[3 * n]
    into = [pltpu.make_async_copy(src[k], held[k], sem.at[0, k]) for k in range(n)]
    out = [pltpu.make_async_copy(held[k], dst[k], sem.at[1, k]) for k in range(n)]
    for made in into:
        made.start()
    for k in range(n):
        into[k].wait()
        out[k].start()
    for made in out:
        made.wait()


def publish(*arrays):
    n = len(arrays)
    return pl.pallas_call(
        functools.partial(publish_kernel, n),
        out_shape=[jax.ShapeDtypeStruct(v.shape, v.dtype) for v in arrays],
        in_specs=[ANY] * n,
        out_specs=[ANY] * n,
        scratch_shapes=[pltpu.VMEM(v.shape, v.dtype) for v in arrays]
        + [pltpu.SemaphoreType.DMA((2, n))],
        compiler_params=pltpu.CompilerParams(vmem_limit_bytes=VMEM_BYTES),
        name="publish",
    )(*arrays)


def with_kernel(inputs, w_conv_up, w_gate_up, w_down, taps, conv_bias, cotangent):
    n, t = lax.axis_size("fs"), lax.axis_size("tp")
    rows = inputs.shape[0]
    shard, width = w_conv_up.shape
    ca = -(-width // (2 * LANES)) * LANES
    shape = jax.ShapeDtypeStruct
    scratch = {**buffers(n, t, shard, width, rows, ca), **semaphores(n, t)}
    acts = [v.T.reshape(2, shard, rows) for v in (inputs, cotangent)]
    got = pl.pallas_call(
        functools.partial(layer_kernel, n, t, tuple(scratch)),
        out_shape=[
            shape((2, shard, rows), jnp.bfloat16),
            shape((shard, width), jnp.float32),
            shape((width,), jnp.float32),
            shape((TAPS, t * width), jnp.float32),
            shape((t * width,), jnp.float32),
        ],
        in_specs=[ANY] * 7,
        out_specs=[ANY] * 5,
        scratch_shapes=list(scratch.values()),
        compiler_params=pltpu.CompilerParams(
            collective_id=0, has_side_effects=True, vmem_limit_bytes=VMEM_BYTES
        ),
        name="layer",
    )(w_down.T, w_conv_up, w_gate_up, *acts, taps, conv_bias)
    grad_inputs, *others = publish(*got)
    return (grad_inputs.reshape(-1, rows).T, *others)


def per_device(inputs, w_conv_up, *rest):
    n, t = lax.axis_size("fs"), lax.axis_size("tp")
    shard, width = w_conv_up.shape
    rows, features = inputs.shape
    fits = n == 8 and t == 4 and features == 2 * shard
    aligned = shard % 8 == 0 and rows % LANES == 0 and width > LANES
    chosen = with_kernel if fits and aligned else with_collectives
    return chosen(inputs, w_conv_up, *rest)


def solution(mesh):
    return jax.shard_map(
        per_device,
        mesh=mesh,
        in_specs=(
            P("fs", "tp"),
            P("fs", "tp"),
            P("fs", "tp"),
            P("tp", "fs"),
            P(),
            P(),
            P("fs", "tp"),
        ),
        out_specs=(P("fs", "tp"), P("fs", "tp"), P("tp"), P(), P()),
        check_vma=False,
    )
```

```python
import functools
import math

import jax
import jax.numpy as jnp
from jax import lax
from jax.experimental import pallas as pl
from jax.experimental.pallas import tpu as pltpu
from jax.sharding import PartitionSpec as P

TAPS = 3
LANES = 128
MESH = pl.DeviceIdType.MESH
VMEM_BYTES = 63 * 1024 * 1024
ANY = pl.BlockSpec(memory_space=pl.ANY)


def shifted(block, axis, distance):
    devices = range(lax.axis_size(axis))
    route = [(i - distance, i) for i in devices if i - distance in devices]
    return lax.ppermute(block, axis, route)


def gelu_parts(value):
    normal_cdf = 0.5 * (1.0 + jax.scipy.special.erf(value / math.sqrt(2.0)))
    density = jnp.exp(-0.5 * value * value) / math.sqrt(2.0 * math.pi)
    return (value * normal_cdf, normal_cdf + value * density)


def with_collectives(inputs, w_conv_up, w_gate_up, w_down, taps, conv_bias, cotangent):
    span = TAPS - 1
    rows = inputs.shape[0]
    width = w_conv_up.shape[1]
    col_start = lax.axis_index("tp") * width
    taps_own = lax.dynamic_slice_in_dim(taps, col_start, width, 1)
    bias_own = lax.dynamic_slice_in_dim(conv_bias, col_start, width, 0)
    features, cot_full = (
        lax.all_gather(inputs, "tp", axis=1, tiled=True),
        lax.all_gather(cotangent, "tp", axis=1, tiled=True),
    )
    conv_weight, gate_weight = (
        lax.all_gather(w_conv_up, "fs", axis=0, tiled=True),
        lax.all_gather(w_gate_up, "fs", axis=0, tiled=True),
    )
    columns = cot_full
    d_hidden = lax.dot_general(
        columns,
        lax.all_gather(w_down, "fs", axis=1, tiled=True),
        (((1,), (1,)), ((), ())),
        preferred_element_type=jnp.float32,
    ).astype(jnp.bfloat16)
    up_a = jnp.dot(features, conv_weight, preferred_element_type=jnp.float32).astype(jnp.bfloat16)
    up_b = jnp.dot(features, gate_weight, preferred_element_type=jnp.float32).astype(jnp.bfloat16)
    earlier = shifted(up_a[rows - span :], "fs", 1)
    extended = jnp.concatenate([earlier, up_a], 0).astype(jnp.float32)
    conv_out = bias_own[None, :] + sum(
        (taps_own[i][None, :] * extended[i : i + rows] for i in range(TAPS))
    )
    gelu_value, gelu_slope = gelu_parts(conv_out)
    hidden_grad = d_hidden.astype(jnp.float32)
    d_conv = hidden_grad * up_b.astype(jnp.float32) * gelu_slope
    d_up_b = (hidden_grad * gelu_value).astype(jnp.bfloat16)
    later = shifted(d_conv[:span], "fs", -1)
    d_extended = jnp.concatenate([d_conv, later], 0)
    d_up_a = sum(
        (taps_own[i][None, :] * d_extended[span - i : span - i + rows] for i in range(TAPS))
    ).astype(jnp.bfloat16)
    tap_terms = [jnp.sum(d_conv * extended[i : i + rows], axis=0) for i in range(TAPS)]
    column_part = jnp.stack(tap_terms + [jnp.sum(d_conv, axis=0)], 0)
    contract = (((1,), (1,)), ((), ()))
    partial_sum = lax.dot_general(d_up_a, conv_weight, contract, preferred_element_type=jnp.float32)
    partial_sum = partial_sum + lax.dot_general(
        d_up_b, gate_weight, contract, preferred_element_type=jnp.float32
    )
    grad_inputs = lax.psum_scatter(
        partial_sum.astype(jnp.bfloat16), "tp", scatter_dimension=1, tiled=True
    )
    columns = features
    grad_conv_up = lax.psum_scatter(
        lax.dot_general(
            columns, d_up_a, (((0,), (0,)), ((), ())), preferred_element_type=jnp.float32
        ),
        "fs",
        scatter_dimension=0,
        tiled=True,
    )
    squares = jnp.sum(grad_conv_up * grad_conv_up, axis=0)
    placed = jnp.zeros((TAPS + 1, width * lax.axis_size("tp")), jnp.float32)
    placed = lax.dynamic_update_slice_in_dim(placed, column_part, col_start, 1)
    full_columns = lax.psum(placed, ("fs", "tp"))
    unit_norms = lax.psum(squares, "fs")
    return (grad_inputs, grad_conv_up, unit_norms, full_columns[:TAPS], full_columns[TAPS])


def greet(peers):
    barrier = pltpu.get_barrier_semaphore()
    for peer in peers:
        pl.semaphore_signal(barrier, inc=1, device_id=peer, device_id_type=MESH)


def greeted(peers):
    pl.semaphore_wait(pltpu.get_barrier_semaphore(), len(peers))


def dot(a, b, da, db):
    return lax.dot_general(
        a, b, (((da,), (db,)), ((), ())), preferred_element_type=jnp.float32
    )


def rounded(value):
    return value.astype(jnp.bfloat16).astype(jnp.float32)


def folded_rows(rows):
    return -(-rows // 32) * 16


def buffers(n, t, shard, width, rows, ca):
    b16, f32 = jnp.bfloat16, jnp.float32
    full, fold = ca // LANES - 1, folded_rows(shard)
    return dict(
        wv=pltpu.VMEM((3, shard, width), b16),
        taps_v=pltpu.VMEM((TAPS, t * width), f32),
        bias_v=pltpu.VMEM((t * width,), f32),
        i_v=pltpu.VMEM((2, shard, rows), b16),
        g_v=pltpu.VMEM((shard, width), f32),
        norm_v=pltpu.VMEM((width,), f32),
        taps_w=pltpu.VMEM((TAPS, t * width), f32),
        bias_w=pltpu.VMEM((t * width,), f32),
        stage=pltpu.VMEM((2, 3, full, shard, LANES), b16),
        stage_end=pltpu.VMEM((3, shard, LANES), b16),
        stage_fold=pltpu.VMEM((3, fold, LANES), b16),
        wmain=pltpu.VMEM((3, n, full, shard, LANES), b16),
        wend=pltpu.VMEM((3, n, shard, LANES), b16),
        wfold=pltpu.VMEM((3, n, fold, LANES), b16),
        abuf=pltpu.VMEM((2, 2, n, shard, rows), b16),
        tot=pltpu.VMEM((3, 2, rows + 8, ca), f32),
        halo_up=pltpu.VMEM((2, 8, ca), f32),
        halo_dc=pltpu.VMEM((2, 8, ca), f32),
        tb=pltpu.VMEM((8, ca), f32),
        dcv=pltpu.VMEM((2, rows + 8, ca), f32),
        dup=pltpu.VMEM((2, 2, rows, ca), b16),
        col_own=pltpu.VMEM((8, ca), f32),
        col_got=pltpu.VMEM((3, 8, ca), f32),
        col_sum=pltpu.VMEM((8, ca), f32),
        col_all=pltpu.VMEM((t, 2, 8, ca), f32),
        ysend=pltpu.VMEM((4, shard, ca), b16),
        yrecv=pltpu.VMEM((4, shard, ca), b16),
        gown=pltpu.VMEM((4, shard, ca), f32),
        zsend=pltpu.VMEM((3, shard, ca), b16),
        zrecv=pltpu.VMEM((4, shard, ca), b16),
        csend=pltpu.VMEM((8, shard, rows), b16),
        crecv=pltpu.VMEM((8, shard, rows), b16),
        pown=pltpu.VMEM((8, shard, rows), f32),
        xsend=pltpu.VMEM((4, shard, rows), b16),
        xrecv=pltpu.VMEM((4, shard, rows), b16),
        psend=pltpu.VMEM((2, shard, rows), b16),
        precv=pltpu.VMEM((2, shard, rows), b16),
        norm_own=pltpu.VMEM((8, ca), f32),
        norm_all=pltpu.VMEM((n, 8, ca), f32),
    )


def semaphores(n, t):
    shapes = dict(
        wz=(3, 3), wy=(3, 4), ez=(3, 3), ey=(3, 4), az=(4,), ax=(2, 4), ac=(4, 4), hu=(2,), hd=(2,),
        c1=(3,), c2=(2 * t - 1,), gy=(4, 2), gz=(4, 2), pc=(8,), px=(4,), pz=(2,), nm=(n - 1,),
    )
    dma = pltpu.SemaphoreType.DMA
    local = dict(ld=dma((9,)), st=dma((6,)))
    return local | {name + end: dma(s) for name, s in shapes.items() for end in ("_s", "_r")}


def layer_kernel(n, t, names, *refs):
    w_in, acts, taps_in, bias_in = refs[:3], refs[3:5], refs[5], refs[6]
    outs = refs[7:12]
    m = dict(zip(names, refs[12:]))
    stage, stage_end, stage_fold = m["stage"], m["stage_end"], m["stage_fold"]
    wmain, wend, wfold, abuf, tot = m["wmain"], m["wend"], m["wfold"], m["abuf"], m["tot"]
    dcv, dup, tb = m["dcv"], m["dup"], m["tb"]
    w, taps, bias = m["wv"], m["taps_v"], m["bias_v"]
    shard, width = w.shape[1:]
    full, fold = stage.shape[2], stage_fold.shape[1]
    ca = (full + 1) * LANES
    cb = width - ca
    odd = cb - full * LANES
    rows = acts[0].shape[2]
    me, mine = lax.axis_index("fs"), lax.axis_index("tp")
    z, y = me // 2, lax.rem(me, 2)
    x, c = mine // 2, lax.rem(mine, 2)
    l = lax.rem(z, 2)
    upper = z // 2
    zp = z + 1 - 2 * l
    zo = 3 - z
    far = 3 - zp
    inner_i = lax.rem((z + 1) // 2, 2)
    inner = inner_i == 1
    outer = inner_i == 0
    across = {"fs": z * 2 + 1 - y}
    pair = {"fs": zp * 2 + y}
    x_dev = {"tp": (1 - x) * 2 + c}
    twin = {"tp": x * 2 + 1 - c}
    x_tp = (1 - x) * 2 + c
    line = [zp, 2 - upper, 3 * (1 - upper)]
    started, guarded = [], []

    def copy(name, at, src, dst, to, slot=None):
        slot = at if slot is None else slot
        return pltpu.make_async_remote_copy(
            src_ref=src, dst_ref=dst,
            send_sem=m[name + "_s"].at[at], recv_sem=m[name + "_r"].at[slot],
            device_id=to, device_id_type=MESH,
        )

    def push(*args, **kw):
        made = copy(*args, **kw)
        made.start()
        started.append(made)
        return made

    def push_if(flag, *args, **kw):
        made = copy(*args, **kw)
        pl.when(flag)(made.start)
        guarded.append((flag, made))

    def put(i):
        for k in range(full):
            at = k * LANES
            stage[0, i, k] = w[i, :, at : at + LANES]
            stage[1, i, k] = w[i, :, ca + at : ca + at + LANES]
        end = w[i, :, ca + full * LANES :]
        stage_end[i] = w[i, :, full * LANES : ca]
        stage_fold[i] = jnp.zeros((fold, LANES), jnp.bfloat16)
        stage_fold[i, :, :odd] = end[:fold]
        stage_fold[i, : shard - fold, odd:] = end[fold:]
        wmain[i, me] = stage[1 - inner_i, i]

        @pl.when(inner)
        def _():
            wend[i, me] = stage_end[i]

        @pl.when(outer)
        def _():
            wend[i, me] = jnp.zeros((shard, LANES), jnp.bfloat16)
            wend[i, me, :, :odd] = end

    def unfold(i, k):
        both = wfold[i, k].astype(jnp.float32)
        low = lax.broadcasted_iota(jnp.int32, both.shape, 1) < odd
        first = jnp.where(low, both, 0.0).astype(jnp.bfloat16)
        second = jnp.where(low, pltpu.roll(both, LANES - odd, 1), 0.0).astype(jnp.bfloat16)
        wend[i, k, :fold] = first
        wend[i, k, fold:] = second[: shard - fold]

    def weight(i, k):
        return jnp.concatenate([wmain[i, k, c] for c in range(full)] + [wend[i, k]], axis=1)

    others = [{"fs": lax.rem(me + k, n)} for k in range(1, n)]
    others += [{"tp": lax.rem(mine + k, t)} for k in range(1, t)]
    others += [{"fs": zp * 2 + y, "tp": lax.rem(mine + k, t)} for k in range(1, t)]
    greet(others)
    loads = []

    def load(src, dst):
        made = pltpu.make_async_copy(src, dst, m["ld"].at[len(loads)])
        made.start()
        loads.append(made)

    for i in range(3):
        load(w_in[i], w.at[i])
    for a in range(2):
        for half in range(2):
            load(acts[a].at[half], abuf.at[a, l, 2 * mine + half])
    load(taps_in, taps)
    load(bias_in, bias)
    for i in range(3):
        loads[i].wait()
        put(i)
    for made in loads[3:]:
        made.wait()
    tb[...] = jnp.zeros(tb.shape, jnp.float32)
    for p in range(t):
        for flag, start, size in ((inner, 0, ca), (outer, ca, cb)):
            @pl.when(jnp.logical_and(mine == p, flag))
            def _(p=p, start=start, size=size):
                at = p * width + start
                tb[0:3, 0:size] = taps[:, at : at + size]
                tb[3:4, 0:size] = bias[at : at + size].reshape(1, size)

    greeted(others)

    quarter = [(1, 0), (1, 1), (0, 0), (0, 1)]
    own_act = [abuf.at[a, l, 2 * mine + half] for a, half in quarter]
    pair_act = [abuf.at[a, 1 - l, 2 * mine + half] for a, half in quarter]
    x_act = [abuf.at[a, l, 2 * x_tp + half] for a, half in quarter]
    xp_act = [abuf.at[a, 1 - l, 2 * x_tp + half] for a, half in quarter]
    az, ax, ac, wz, wy = {}, {}, {}, {}, {}

    def send_act(q):
        az[q] = push("az", (q,), own_act[q], own_act[q], pair)
        ax[0, q] = push("ax", (0, q), own_act[q], own_act[q], x_dev)
        ac[0, q] = push("ac", (0, q), own_act[q], own_act[q], twin)

    def send_w(i, j):
        own, own_end, own_fold = wmain.at[i, me], wend.at[i, me], wfold.at[i, me]
        ends, folds = stage_end.at[i], stage_fold.at[i]
        if j == 3:
            wy[i, 3] = push("wy", (i, 3), own, own, across)
            push_if(inner, "ey", (i, 3), ends, own_end, across)
            push_if(outer, "ey", (i, 3), folds, own_fold, across)
            return
        to = {"fs": line[j] * 2 + y}
        at = (i, 0 if j == 0 else 2 - inner_i)
        push("wz", (i, j), stage.at[inner_i if j == 0 else j - 1, i], own, to, slot=at)
        if j == 0:
            push_if(outer, "ez", (i, j), ends, own_end, to, slot=at)
            push_if(inner, "ez", (i, j), folds, own_fold, to, slot=at)
        elif j == 1:
            push("ez", (i, j), ends, own_end, to, slot=at)
        else:
            push("ez", (i, j), folds, own_fold, to, slot=at)

    def pass_w(i, j):
        k = line[j] * 2 + y
        slot = wmain.at[i, k]
        copy("wz", (i, j), slot, slot, pair).wait_recv()
        wy[i, j] = push("wy", (i, j), slot, slot, across)
        for flag, ref in ((inner, wend.at[i, k]), (outer, wfold.at[i, k])):
            pl.when(flag)(copy("ez", (i, j), ref, ref, pair).wait_recv)
            push_if(flag, "ey", (i, j), ref, ref, across)

    def pass_pair(q):
        az[q].wait_recv()
        ax[1, q] = push("ax", (1, q), pair_act[q], pair_act[q], x_dev)
        ac[1, q] = push("ac", (1, q), pair_act[q], pair_act[q], twin)

    def pass_x(way, q):
        ax[way, q].wait_recv()
        ref = (x_act, xp_act)[way][q]
        ac[2 + way, q] = push("ac", (2 + way, q), ref, ref, twin)

    def multiply(i, zz, b, halves, fresh):
        a = 1 if i == 0 else 0
        product = 0.0
        for half in halves:
            k = 2 * zz + half
            product = product + dot(abuf[a, b, k], weight(i, k), 0, 0)
        if fresh:
            tot[i, b, 8:, :] = product
        else:
            tot[i, b, 8:, :] = tot[i, b, 8:, :] + product

    arrived, acts_seen = set(), set()

    def compute(i, j, which, *only):
        halves = only or (0, 1)
        if (i, j) not in arrived:
            arrived.add((i, j))
            wy[i, j].wait_recv()
            zz = z if j == 3 else line[j]
            k = zz * 2 + 1 - y

            @pl.when(inner)
            def _():
                copy("ey", (i, j), wend.at[i, k], wend.at[i, k], across).wait_recv()

            @pl.when(outer)
            def _():
                copy("ey", (i, j), wfold.at[i, k], wfold.at[i, k], across).wait_recv()
                unfold(i, k)
                if j != 3:
                    unfold(i, zz * 2 + y)

        for q in [half + (2 if i else 0) for half in halves]:
            for s in (0, 2) if which == 0 else (1, 3):
                if (s, q) not in acts_seen:
                    acts_seen.add((s, q))
                    ac[s, q].wait_recv()
        fresh = j == 3 and halves[0] == 0
        multiply(i, z if j == 3 else line[j], l if which == 0 else 1 - l, halves, fresh)

    sending = (
        "a0 a1 w03 w02", "w01 w13 a2 w00", "w12 w11 w23 a3", "w22 w21 w10 w20",
    )
    for item in " ".join(sending).split():
        if item[0] == "a":
            send_act(int(item[1]))
        else:
            send_w(int(item[1]), int(item[2]))
    passing = (
        "x00 w01 p0 x01", "c030 x02 w02 p1", "c010 x03 w11 c130", "c230 x10 p2 c020",
        "w12 x11 c110 c031", "w00 c011 w21 x12", "c120 c021 c1310 c1110", "p3 w22 c2310 c1210",
        "c000 c001 w10 c210", "c2110 x13 c220 c1311", "c1111 w20 c1211 c100", "c101",
    )
    for item in " ".join(passing).split():
        at = [int(v) for v in item[1:]]
        dict(x=pass_x, w=pass_w, p=pass_pair, c=compute)[item[0]](*at)
    for b in range(2):
        edge, where = tot.at[1, b, pl.ds(rows, 8)], m["halo_up"]
        if b == 0:
            push("hu", (0,), edge, where.at[y], across, slot=(y,))
        else:
            hu_near = copy("hu", (1,), edge, where.at[1], across)
            hu_far = copy("hu", (1,), edge, where.at[0], {"fs": zo * 2}, slot=(0,))
            pl.when(y == 0)(hu_near.start)
            pl.when(jnp.logical_and(y == 1, upper == 0))(hu_far.start)

    span = 32
    steps = rows // span

    def row(k):
        return tb[k : k + 1, :]

    def gelu_rows(b, r):
        at = pl.multiple_of(r * span, span)
        around = rounded(tot[1, b, pl.ds(at, span + 8), :])
        value = row(3) + row(0) * around[6 : 6 + span]
        value = value + row(1) * around[7 : 7 + span] + row(2) * around[8 : 8 + span]
        cdf = 0.5 * (1.0 + lax.erf(value * (1.0 / math.sqrt(2.0))))
        density = jnp.exp(-0.5 * value * value) * (1.0 / math.sqrt(2.0 * math.pi))
        hidden = rounded(tot[0, b, pl.ds(at + 8, span), :])
        dup[1, b, pl.ds(at, span), :] = (hidden * (value * cdf)).astype(jnp.bfloat16)
        dcv[b, pl.ds(at, span), :] = hidden * (cdf + value * density)

    @pl.loop(0, 2 * (steps - 1))
    def _(k):
        gelu_rows(lax.rem(k, 2), 1 + k // 2)

    compute(2, 3, 1, 1)
    compute(2, 1, 1, 1)
    compute(2, 2, 1)
    has_before = jnp.logical_or(y == 1, upper == 1)
    wait_up = [copy("hu", (b,), m["halo_up"].at[b], m["halo_up"].at[b], across) for b in range(2)]
    wait_up[1].wait_recv()
    pl.when(has_before)(wait_up[0].wait_recv)
    tot[1, 1, 0:8, :] = m["halo_up"][1]

    @pl.when(has_before)
    def _():
        tot[1, 0, 0:8, :] = m["halo_up"][0]

    @pl.when(jnp.logical_not(has_before))
    def _():
        tot[1, 0, 0:8, :] = jnp.zeros((8, ca), jnp.float32)

    @pl.loop(0, 2)
    def _(b):
        gelu_rows(b, 0)

    for which in range(2):
        compute(2, 0, which)

    def grad_rows(b, r, sums):
        at = pl.multiple_of(r * span, span)
        grad = dcv[b, pl.ds(at, span), :] * rounded(tot[2, b, pl.ds(at + 8, span), :])
        dcv[b, pl.ds(at, span), :] = grad
        around = rounded(tot[1, b, pl.ds(at, span + 8), :])

        def folded(value):
            total = value[0:8]
            for k in range(8, span, 8):
                total = total + value[k : k + 8]
            return total

        terms = [folded(grad * around[6 + i : 6 + i + span]) for i in range(3)] + [folded(grad)]
        return tuple(s + v for s, v in zip(sums, terms))

    sums = tuple(jnp.zeros((8, ca), jnp.float32) for _ in range(4))
    sums = lax.fori_loop(0, 2, lambda b, s: grad_rows(b, 0, s), sums)
    edge = dcv.at[0, pl.ds(0, 8)]
    hd_near = copy("hd", (0,), edge, m["halo_dc"].at[0], across)
    hd_far = copy("hd", (0,), edge, m["halo_dc"].at[1], {"fs": zo * 2 + 1}, slot=(1,))
    pl.when(y == 1)(hd_near.start)
    pl.when(jnp.logical_and(y == 0, upper == 1))(hd_far.start)
    push("hd", (1,), dcv.at[1, pl.ds(0, 8)], m["halo_dc"].at[y], across, slot=(y,))
    sums = lax.fori_loop(
        0, 2 * (steps - 1), lambda k, s: grad_rows(lax.rem(k, 2), 1 + k // 2, s), sums
    )
    m["col_own"][4:8, :] = jnp.zeros((4, ca), jnp.float32)
    for k in range(4):
        m["col_own"][k : k + 1, :] = jnp.sum(sums[k], axis=0, keepdims=True)
    group = [across, {"fs": zo * 2 + y}, {"fs": zo * 2 + 1 - y}]
    c1 = [push("c1", (k,), m["col_own"], m["col_got"].at[k], group[k]) for k in range(3)]

    def shift_rows(b, r):
        at = pl.multiple_of(r * span, span)
        ahead = dcv[b, pl.ds(at, span + 8), :]
        total = row(0) * ahead[2 : 2 + span] + row(1) * ahead[1 : 1 + span]
        total = total + row(2) * ahead[0:span]
        dup[0, b, pl.ds(at, span), :] = total.astype(jnp.bfloat16)

    @pl.loop(0, 2 * (steps - 1))
    def _(k):
        shift_rows(lax.rem(k, 2), k // 2)

    has_next = jnp.logical_or(y == 0, upper == 0)
    wait_dc = [copy("hd", (b,), m["halo_dc"].at[b], m["halo_dc"].at[b], across) for b in range(2)]
    wait_dc[0].wait_recv()
    pl.when(has_next)(wait_dc[1].wait_recv)
    dcv[0, rows : rows + 8, :] = m["halo_dc"][0]

    @pl.when(has_next)
    def _():
        dcv[1, rows : rows + 8, :] = m["halo_dc"][1]

    @pl.when(jnp.logical_not(has_next))
    def _():
        dcv[1, rows : rows + 8, :] = jnp.zeros((8, ca), jnp.float32)

    @pl.loop(0, 2)
    def _(b):
        shift_rows(b, steps - 1)

    def weight_grad(zz, yy):
        k = 2 * zz + yy
        return dot(abuf[0, 0, k], dup[0, 0], 1, 0) + dot(abuf[0, 1, k], dup[0, 1], 1, 0)

    def input_grad(b, k):
        return dot(weight(1, k), dup[0, b], 1, 1) + dot(weight(2, k), dup[1, b], 1, 1)

    b16, f32 = jnp.bfloat16, jnp.float32
    order = [far, zo, zp, z]
    ysend, yrecv, gown, zsend, zrecv = (m[k] for k in ("ysend", "yrecv", "gown", "zsend", "zrecv"))
    csend, crecv, pown, xsend, xrecv = (m[k] for k in ("csend", "crecv", "pown", "xsend", "xrecv"))
    psend, precv = m["psend"], m["precv"]
    gy, pc, px, pz = {}, {}, {}, {}

    def spot(bi, xi, half):
        return bi * 4 + xi * 2 + half

    def to_twin(bi, xi, half):
        b, xx, at = (1 - l, l)[bi], (1 - x, x)[xi], spot(bi, xi, half)
        csend[at] = input_grad(b, 2 * (xx * 2 + 1 - c) + half).astype(b16)
        pc[at] = push("pc", (at,), csend.at[at], crecv.at[at], twin)

    def keep(bi, xi, half):
        b, xx, at = (1 - l, l)[bi], (1 - x, x)[xi], spot(bi, xi, half)
        pown[at] = input_grad(b, 2 * (xx * 2 + c) + half)

    def to_x(bi, half):
        at, to = spot(bi, 0, half), bi * 2 + half
        pc[at].wait_recv()
        xsend[to] = (pown[at] + crecv[at].astype(f32)).astype(b16)
        px[to] = push("px", (to,), xsend.at[to], xrecv.at[to], x_dev)

    def to_pair(half):
        at = spot(0, 1, half)
        pc[at].wait_recv()
        px[half].wait_recv()
        total = pown[at] + crecv[at].astype(f32) + xrecv[half].astype(f32)
        psend[half] = total.astype(b16)
        pz[half] = push("pz", (half,), psend.at[half], precv.at[half], pair)

    i_v, g_v, norm_v, taps_w, bias_w = (
        m[k] for k in ("i_v", "g_v", "norm_v", "taps_w", "bias_w")
    )
    stores = []

    def store(src, dst):
        made = pltpu.make_async_copy(src, dst, m["st"].at[len(stores)])
        made.start()
        stores.append(made)

    def finish(half):
        at = spot(1, 1, half)
        pc[at].wait_recv()
        px[2 + half].wait_recv()
        pz[half].wait_recv()
        total = pown[at] + crecv[at].astype(f32)
        total = total + xrecv[2 + half].astype(f32) + precv[half].astype(f32)
        i_v[half] = total.astype(b16)
        store(i_v.at[half], outs[0].at[half])

    first_rows = -(-shard // 16) * 8
    parts = (pl.ds(0, first_rows), pl.ds(first_rows, shard - first_rows))
    first_to = inner_i * zo + (1 - inner_i) * far
    first_at = 3 - 2 * inner_i
    last_at = 2 - inner_i

    def to_across(k):
        ysend[k] = weight_grad(order[k], 1 - y).astype(b16)
        for s, at in enumerate(parts):
            gy[k, s] = push("gy", (k, s), ysend.at[k, at], yrecv.at[k, at], across)

    def own(k):
        gown[k] = weight_grad(order[k], y)

    def add_across(k, s):
        gy[k, s].wait_recv()
        at = parts[s]
        gown[k, at, :] = gown[k, at, :] + yrecv[k, at, :].astype(f32)

    def to_line(k, s, dev, slot):
        at = parts[s]
        push(
            "gz", (k, s), zsend.at[k, at], zrecv.at[slot, at], {"fs": dev * 2 + y}, slot=(slot, s)
        )

    def got_line(k, s):
        at = parts[s]
        copy("gz", (k, s), zrecv.at[k, at], zrecv.at[k, at], across).wait_recv()

    def send_columns():
        for k in range(3):
            c1[k].wait_recv()
        got = m["col_got"]
        m["col_sum"][...] = (m["col_own"][...] + got[0]) + (got[1] + got[2])
        place = m["col_all"].at[mine, 1 - inner_i]
        place[...] = m["col_sum"][...]
        for k in range(1, 2 * t):
            tp = lax.rem(mine + k // 2, t)
            to = {"fs": (zp if k % 2 else z) * 2 + y, "tp": tp}
            c2.append(push("c2", (k - 1,), m["col_sum"], place, to))

    c2 = []
    to_across(0)
    to_twin(0, 0, 0)
    to_across(1)
    to_twin(0, 0, 1)
    keep(0, 0, 0)
    send_columns()
    to_x(0, 0)
    keep(0, 0, 1)
    to_x(0, 1)
    to_across(2)
    to_across(3)
    own(0)
    for s in range(2):
        add_across(0, s)
        zsend[0, parts[s], :] = gown[0, parts[s], :].astype(b16)
        to_line(0, s, first_to, first_at)
    own(1)
    to_twin(1, 0, 0)
    to_twin(1, 0, 1)
    keep(1, 0, 0)
    to_x(1, 0)
    for s in range(2):
        add_across(1, s)
        zsend[1, parts[s], :] = gown[1, parts[s], :].astype(b16)
        to_line(1, s, zo, 0)
    keep(1, 0, 1)
    to_x(1, 1)
    own(2)
    to_twin(0, 1, 0)
    to_twin(0, 1, 1)
    keep(0, 1, 0)
    keep(0, 1, 1)
    to_pair(0)
    for s in range(2):
        add_across(2, s)

        @pl.when(outer)
        def _(at=parts[s]):
            zsend[2, at, :] = gown[2, at, :].astype(b16)

        @pl.when(inner)
        def _(s=s, at=parts[s]):
            got_line(1, s)
            zsend[2, at, :] = (gown[2, at, :] + zrecv[1, at, :].astype(f32)).astype(b16)

        to_line(2, s, zp, last_at)
    to_pair(1)
    own(3)
    for half in range(2):
        to_twin(1, 1, half)
        keep(1, 1, half)
    for s in range(2):
        add_across(3, s)
        got_line(0, s)
    norm_own, norm_all = m["norm_own"], m["norm_all"]
    norm_own[...] = jnp.zeros(norm_own.shape, f32)

    def settle(k, value):
        g_v[:, k * ca : k * ca + (cb if k else ca)] = value[:, : (cb if k else ca)]
        norm_own[k : k + 1, :] = jnp.sum(value * value, axis=0, keepdims=True)

    @pl.when(inner)
    def _():
        settle(0, gown[3] + zrecv[0].astype(f32))
        for s in range(2):
            got_line(2, s)
            got_line(3, s)
        settle(1, zrecv[2].astype(f32) + zrecv[3].astype(f32))

    @pl.when(outer)
    def _():
        settle(1, gown[3] + zrecv[0].astype(f32))
        for s in range(2):
            got_line(1, s)
        settle(0, zrecv[1].astype(f32))

    norms = [
        push("nm", (k,), norm_own, norm_all.at[me], others[k]) for k in range(n - 1)
    ]
    store(g_v, outs[1])
    finish(0)
    for copy_in in c2:
        copy_in.wait_recv()
    whole = m["col_all"]
    for p in range(t):
        at = p * width
        taps_w[:, at : at + ca] = whole[p, 0, 0:3, :]
        taps_w[:, at + ca : at + width] = whole[p, 1, 0:3, :cb]
        bias_w[at : at + ca] = whole[p, 0, 3, :]
        bias_w[at + ca : at + width] = whole[p, 1, 3, :cb]
    store(taps_w, outs[3])
    store(bias_w, outs[4])
    finish(1)
    for copy_in in norms:
        copy_in.wait_recv()
    norm_all[me] = norm_own[...]
    total = norm_all[0]
    for k in range(1, n):
        total = total + norm_all[k]
    norm_v[:ca] = total[0]
    norm_v[ca:] = total[1, :cb]
    store(norm_v, outs[2])
    for made in started:
        made.wait_send()
    for made in stores:
        made.wait()
    for flag, made in guarded:
        pl.when(flag)(made.wait_send)
    pl.when(y == 0)(hu_near.wait_send)
    pl.when(jnp.logical_and(y == 1, upper == 0))(hu_far.wait_send)
    pl.when(y == 1)(hd_near.wait_send)
    pl.when(jnp.logical_and(y == 0, upper == 1))(hd_far.wait_send)


def publish_kernel(n, *refs):
    src, dst, held, sem = refs[:n], refs[n : 2 * n], refs[2 * n : 3 * n], refs[3 * n]
    into = [pltpu.make_async_copy(src[k], held[k], sem.at[0, k]) for k in range(n)]
    out = [pltpu.make_async_copy(held[k], dst[k], sem.at[1, k]) for k in range(n)]
    for made in into:
        made.start()
    for k in range(n):
        into[k].wait()
        out[k].start()
    for made in out:
        made.wait()


def publish(*arrays):
    n = len(arrays)
    return pl.pallas_call(
        functools.partial(publish_kernel, n),
        out_shape=[jax.ShapeDtypeStruct(v.shape, v.dtype) for v in arrays],
        in_specs=[ANY] * n,
        out_specs=[ANY] * n,
        scratch_shapes=[pltpu.VMEM(v.shape, v.dtype) for v in arrays]
        + [pltpu.SemaphoreType.DMA((2, n))],
        compiler_params=pltpu.CompilerParams(vmem_limit_bytes=VMEM_BYTES),
        name="publish",
    )(*arrays)


def with_kernel(inputs, w_conv_up, w_gate_up, w_down, taps, conv_bias, cotangent):
    n, t = lax.axis_size("fs"), lax.axis_size("tp")
    rows = inputs.shape[0]
    shard, width = w_conv_up.shape
    ca = -(-width // (2 * LANES)) * LANES
    shape = jax.ShapeDtypeStruct
    scratch = {**buffers(n, t, shard, width, rows, ca), **semaphores(n, t)}
    acts = [v.T.reshape(2, shard, rows) for v in (inputs, cotangent)]
    got = pl.pallas_call(
        functools.partial(layer_kernel, n, t, tuple(scratch)),
        out_shape=[
            shape((2, shard, rows), jnp.bfloat16),
            shape((shard, width), jnp.float32),
            shape((width,), jnp.float32),
            shape((TAPS, t * width), jnp.float32),
            shape((t * width,), jnp.float32),
        ],
        in_specs=[ANY] * 7,
        out_specs=[ANY] * 5,
        scratch_shapes=list(scratch.values()),
        compiler_params=pltpu.CompilerParams(
            collective_id=0, has_side_effects=True, vmem_limit_bytes=VMEM_BYTES
        ),
        name="layer",
    )(w_down.T, w_conv_up, w_gate_up, *acts, taps, conv_bias)
    grad_inputs, *others = publish(*got)
    return (grad_inputs.reshape(-1, rows).T, *others)


def per_device(inputs, w_conv_up, *rest):
    n, t = lax.axis_size("fs"), lax.axis_size("tp")
    shard, width = w_conv_up.shape
    rows, features = inputs.shape
    fits = n == 8 and t == 4 and features == 2 * shard
    aligned = shard % 8 == 0 and rows % LANES == 0 and width > 2 * LANES
    aligned = aligned and width % (2 * LANES) == LANES + LANES // 2
    chosen = with_kernel if fits and aligned else with_collectives
    return chosen(inputs, w_conv_up, *rest)


def solution(mesh):
    return jax.shard_map(
        per_device,
        mesh=mesh,
        in_specs=(
            P("fs", "tp"),
            P("fs", "tp"),
            P("fs", "tp"),
            P("tp", "fs"),
            P(),
            P(),
            P("fs", "tp"),
        ),
        out_specs=(P("fs", "tp"), P("fs", "tp"), P("tp"), P(), P()),
        check_vma=False,
    )
```

```python
import functools
import math

import jax
import jax.numpy as jnp
from jax import lax
from jax.experimental import pallas as pl
from jax.experimental.pallas import tpu as pltpu
from jax.sharding import PartitionSpec as P

TAPS = 3
LANES = 128
MESH = pl.DeviceIdType.MESH
VMEM_BYTES = 63 * 1024 * 1024
ANY = pl.BlockSpec(memory_space=pl.ANY)


def shifted(block, axis, distance):
    devices = range(lax.axis_size(axis))
    route = [(i - distance, i) for i in devices if i - distance in devices]
    return lax.ppermute(block, axis, route)


def gelu_parts(value):
    normal_cdf = 0.5 * (1.0 + jax.scipy.special.erf(value / math.sqrt(2.0)))
    density = jnp.exp(-0.5 * value * value) / math.sqrt(2.0 * math.pi)
    return (value * normal_cdf, normal_cdf + value * density)


def with_collectives(inputs, w_conv_up, w_gate_up, w_down, taps, conv_bias, cotangent):
    span = TAPS - 1
    rows = inputs.shape[0]
    width = w_conv_up.shape[1]
    col_start = lax.axis_index("tp") * width
    taps_own = lax.dynamic_slice_in_dim(taps, col_start, width, 1)
    bias_own = lax.dynamic_slice_in_dim(conv_bias, col_start, width, 0)
    features, cot_full = (
        lax.all_gather(inputs, "tp", axis=1, tiled=True),
        lax.all_gather(cotangent, "tp", axis=1, tiled=True),
    )
    conv_weight, gate_weight = (
        lax.all_gather(w_conv_up, "fs", axis=0, tiled=True),
        lax.all_gather(w_gate_up, "fs", axis=0, tiled=True),
    )
    columns = cot_full
    d_hidden = lax.dot_general(
        columns,
        lax.all_gather(w_down, "fs", axis=1, tiled=True),
        (((1,), (1,)), ((), ())),
        preferred_element_type=jnp.float32,
    ).astype(jnp.bfloat16)
    up_a = jnp.dot(features, conv_weight, preferred_element_type=jnp.float32).astype(jnp.bfloat16)
    up_b = jnp.dot(features, gate_weight, preferred_element_type=jnp.float32).astype(jnp.bfloat16)
    earlier = shifted(up_a[rows - span :], "fs", 1)
    extended = jnp.concatenate([earlier, up_a], 0).astype(jnp.float32)
    conv_out = bias_own[None, :] + sum(
        (taps_own[i][None, :] * extended[i : i + rows] for i in range(TAPS))
    )
    gelu_value, gelu_slope = gelu_parts(conv_out)
    hidden_grad = d_hidden.astype(jnp.float32)
    d_conv = hidden_grad * up_b.astype(jnp.float32) * gelu_slope
    d_up_b = (hidden_grad * gelu_value).astype(jnp.bfloat16)
    later = shifted(d_conv[:span], "fs", -1)
    d_extended = jnp.concatenate([d_conv, later], 0)
    d_up_a = sum(
        (taps_own[i][None, :] * d_extended[span - i : span - i + rows] for i in range(TAPS))
    ).astype(jnp.bfloat16)
    tap_terms = [jnp.sum(d_conv * extended[i : i + rows], axis=0) for i in range(TAPS)]
    column_part = jnp.stack(tap_terms + [jnp.sum(d_conv, axis=0)], 0)
    contract = (((1,), (1,)), ((), ()))
    partial_sum = lax.dot_general(d_up_a, conv_weight, contract, preferred_element_type=jnp.float32)
    partial_sum = partial_sum + lax.dot_general(
        d_up_b, gate_weight, contract, preferred_element_type=jnp.float32
    )
    grad_inputs = lax.psum_scatter(
        partial_sum.astype(jnp.bfloat16), "tp", scatter_dimension=1, tiled=True
    )
    columns = features
    grad_conv_up = lax.psum_scatter(
        lax.dot_general(
            columns, d_up_a, (((0,), (0,)), ((), ())), preferred_element_type=jnp.float32
        ),
        "fs",
        scatter_dimension=0,
        tiled=True,
    )
    squares = jnp.sum(grad_conv_up * grad_conv_up, axis=0)
    placed = jnp.zeros((TAPS + 1, width * lax.axis_size("tp")), jnp.float32)
    placed = lax.dynamic_update_slice_in_dim(placed, column_part, col_start, 1)
    full_columns = lax.psum(placed, ("fs", "tp"))
    unit_norms = lax.psum(squares, "fs")
    return (grad_inputs, grad_conv_up, unit_norms, full_columns[:TAPS], full_columns[TAPS])


def greet(peers):
    barrier = pltpu.get_barrier_semaphore()
    for peer in peers:
        pl.semaphore_signal(barrier, inc=1, device_id=peer, device_id_type=MESH)


def greeted(peers):
    pl.semaphore_wait(pltpu.get_barrier_semaphore(), len(peers))


def dot(a, b, da, db):
    return lax.dot_general(
        a, b, (((da,), (db,)), ((), ())), preferred_element_type=jnp.float32
    )


def rounded(value):
    return value.astype(jnp.bfloat16).astype(jnp.float32)


def folded_rows(rows):
    return -(-rows // 32) * 16


def buffers(n, t, shard, width, rows, ca):
    b16, f32 = jnp.bfloat16, jnp.float32
    full, fold = ca // LANES - 1, folded_rows(shard)
    return dict(
        wv=pltpu.VMEM((3, shard, width), b16),
        taps_v=pltpu.VMEM((TAPS, t * width), f32),
        bias_v=pltpu.VMEM((t * width,), f32),
        i_v=pltpu.VMEM((2, shard, rows), b16),
        g_v=pltpu.VMEM((shard, width), f32),
        norm_v=pltpu.VMEM((width,), f32),
        taps_w=pltpu.VMEM((TAPS, t * width), f32),
        bias_w=pltpu.VMEM((t * width,), f32),
        stage=pltpu.VMEM((2, 3, full, shard, LANES), b16),
        stage_end=pltpu.VMEM((3, shard, LANES), b16),
        stage_fold=pltpu.VMEM((3, fold, LANES), b16),
        wmain=pltpu.VMEM((3, n, full, shard, LANES), b16),
        wend=pltpu.VMEM((3, n, shard, LANES), b16),
        wfold=pltpu.VMEM((3, n, fold, LANES), b16),
        abuf=pltpu.VMEM((2, 2, n, shard, rows), b16),
        tot=pltpu.VMEM((3, 2, rows + 8, ca), f32),
        halo_up=pltpu.VMEM((2, 8, ca), f32),
        halo_dc=pltpu.VMEM((2, 8, ca), f32),
        tb=pltpu.VMEM((8, ca), f32),
        dcv=pltpu.VMEM((2, rows + 8, ca), f32),
        dup=pltpu.VMEM((2, 2, rows, ca), b16),
        col_own=pltpu.VMEM((8, ca), f32),
        col_got=pltpu.VMEM((3, 8, ca), f32),
        col_sum=pltpu.VMEM((8, ca), f32),
        col_all=pltpu.VMEM((t, 2, 8, ca), f32),
        ysend=pltpu.VMEM((4, shard, ca), b16),
        yrecv=pltpu.VMEM((4, shard, ca), b16),
        gown=pltpu.VMEM((4, shard, ca), f32),
        zsend=pltpu.VMEM((3, shard, ca), b16),
        zrecv=pltpu.VMEM((4, shard, ca), b16),
        csend=pltpu.VMEM((8, shard, rows), b16),
        crecv=pltpu.VMEM((8, shard, rows), b16),
        pown=pltpu.VMEM((8, shard, rows), f32),
        xsend=pltpu.VMEM((4, shard, rows), b16),
        xrecv=pltpu.VMEM((4, shard, rows), b16),
        psend=pltpu.VMEM((2, shard, rows), b16),
        precv=pltpu.VMEM((2, shard, rows), b16),
        norm_own=pltpu.VMEM((8, ca), f32),
        norm_all=pltpu.VMEM((n, 8, ca), f32),
    )


def semaphores(n, t):
    shapes = dict(
        wz=(3, 3), wy=(3, 4), ez=(3, 3), ey=(3, 4), az=(4,), ax=(2, 4), ac=(4, 4), hu=(2,), hd=(2,),
        c1=(3,), c2=(2 * t - 1,), gy=(4, 2), gz=(4, 2), pc=(8,), px=(4, 2), pz=(2, 2), nm=(n - 1,),
    )
    dma = pltpu.SemaphoreType.DMA
    local = dict(ld=dma((9,)), st=dma((8,)))
    return local | {name + end: dma(s) for name, s in shapes.items() for end in ("_s", "_r")}


def layer_kernel(n, t, names, *refs):
    w_in, acts, taps_in, bias_in = refs[:3], refs[3:5], refs[5], refs[6]
    outs = refs[7:12]
    m = dict(zip(names, refs[12:]))
    stage, stage_end, stage_fold = m["stage"], m["stage_end"], m["stage_fold"]
    wmain, wend, wfold, abuf, tot = m["wmain"], m["wend"], m["wfold"], m["abuf"], m["tot"]
    dcv, dup, tb = m["dcv"], m["dup"], m["tb"]
    w, taps, bias = m["wv"], m["taps_v"], m["bias_v"]
    shard, width = w.shape[1:]
    full, fold = stage.shape[2], stage_fold.shape[1]
    ca = (full + 1) * LANES
    cb = width - ca
    odd = cb - full * LANES
    rows = acts[0].shape[2]
    me, mine = lax.axis_index("fs"), lax.axis_index("tp")
    z, y = me // 2, lax.rem(me, 2)
    x, c = mine // 2, lax.rem(mine, 2)
    l = lax.rem(z, 2)
    upper = z // 2
    zp = z + 1 - 2 * l
    zo = 3 - z
    far = 3 - zp
    inner_i = lax.rem((z + 1) // 2, 2)
    inner = inner_i == 1
    outer = inner_i == 0
    across = {"fs": z * 2 + 1 - y}
    pair = {"fs": zp * 2 + y}
    x_dev = {"tp": (1 - x) * 2 + c}
    twin = {"tp": x * 2 + 1 - c}
    x_tp = (1 - x) * 2 + c
    line = [zp, 2 - upper, 3 * (1 - upper)]
    started, guarded = [], []

    def copy(name, at, src, dst, to, slot=None):
        slot = at if slot is None else slot
        return pltpu.make_async_remote_copy(
            src_ref=src, dst_ref=dst,
            send_sem=m[name + "_s"].at[at], recv_sem=m[name + "_r"].at[slot],
            device_id=to, device_id_type=MESH,
        )

    def push(*args, **kw):
        made = copy(*args, **kw)
        made.start()
        started.append(made)
        return made

    def push_if(flag, *args, **kw):
        made = copy(*args, **kw)
        pl.when(flag)(made.start)
        guarded.append((flag, made))

    def put(i):
        for k in range(full):
            at = k * LANES
            stage[0, i, k] = w[i, :, at : at + LANES]
            stage[1, i, k] = w[i, :, ca + at : ca + at + LANES]
        end = w[i, :, ca + full * LANES :]
        stage_end[i] = w[i, :, full * LANES : ca]
        stage_fold[i] = jnp.zeros((fold, LANES), jnp.bfloat16)
        stage_fold[i, :, :odd] = end[:fold]
        stage_fold[i, : shard - fold, odd:] = end[fold:]
        wmain[i, me] = stage[1 - inner_i, i]

        @pl.when(inner)
        def _():
            wend[i, me] = stage_end[i]

        @pl.when(outer)
        def _():
            wend[i, me] = jnp.zeros((shard, LANES), jnp.bfloat16)
            wend[i, me, :, :odd] = end

    def unfold(i, k):
        both = wfold[i, k].astype(jnp.float32)
        low = lax.broadcasted_iota(jnp.int32, both.shape, 1) < odd
        first = jnp.where(low, both, 0.0).astype(jnp.bfloat16)
        second = jnp.where(low, pltpu.roll(both, LANES - odd, 1), 0.0).astype(jnp.bfloat16)
        wend[i, k, :fold] = first
        wend[i, k, fold:] = second[: shard - fold]

    def weight(i, k):
        return jnp.concatenate([wmain[i, k, c] for c in range(full)] + [wend[i, k]], axis=1)

    others = [{"fs": lax.rem(me + k, n)} for k in range(1, n)]
    others += [{"tp": lax.rem(mine + k, t)} for k in range(1, t)]
    others += [{"fs": zp * 2 + y, "tp": lax.rem(mine + k, t)} for k in range(1, t)]
    greet(others)
    loads = []

    def load(src, dst):
        made = pltpu.make_async_copy(src, dst, m["ld"].at[len(loads)])
        made.start()
        loads.append(made)

    for i in range(3):
        load(w_in[i], w.at[i])
    for a in range(2):
        for half in range(2):
            load(acts[a].at[half], abuf.at[a, l, 2 * mine + half])
    load(taps_in, taps)
    load(bias_in, bias)
    for i in range(3):
        loads[i].wait()
        put(i)
    for made in loads[3:]:
        made.wait()
    tb[...] = jnp.zeros(tb.shape, jnp.float32)
    for p in range(t):
        for flag, start, size in ((inner, 0, ca), (outer, ca, cb)):
            @pl.when(jnp.logical_and(mine == p, flag))
            def _(p=p, start=start, size=size):
                at = p * width + start
                tb[0:3, 0:size] = taps[:, at : at + size]
                tb[3:4, 0:size] = bias[at : at + size].reshape(1, size)

    greeted(others)

    quarter = [(1, 0), (1, 1), (0, 0), (0, 1)]
    own_act = [abuf.at[a, l, 2 * mine + half] for a, half in quarter]
    pair_act = [abuf.at[a, 1 - l, 2 * mine + half] for a, half in quarter]
    x_act = [abuf.at[a, l, 2 * x_tp + half] for a, half in quarter]
    xp_act = [abuf.at[a, 1 - l, 2 * x_tp + half] for a, half in quarter]
    az, ax, ac, wz, wy = {}, {}, {}, {}, {}

    def send_act(q):
        az[q] = push("az", (q,), own_act[q], own_act[q], pair)
        ax[0, q] = push("ax", (0, q), own_act[q], own_act[q], x_dev)
        ac[0, q] = push("ac", (0, q), own_act[q], own_act[q], twin)

    def send_w(i, j):
        own, own_end, own_fold = wmain.at[i, me], wend.at[i, me], wfold.at[i, me]
        ends, folds = stage_end.at[i], stage_fold.at[i]
        if j == 3:
            wy[i, 3] = push("wy", (i, 3), own, own, across)
            push_if(inner, "ey", (i, 3), ends, own_end, across)
            push_if(outer, "ey", (i, 3), folds, own_fold, across)
            return
        to = {"fs": line[j] * 2 + y}
        at = (i, 0 if j == 0 else 2 - inner_i)
        push("wz", (i, j), stage.at[inner_i if j == 0 else j - 1, i], own, to, slot=at)
        if j == 0:
            push_if(outer, "ez", (i, j), ends, own_end, to, slot=at)
            push_if(inner, "ez", (i, j), folds, own_fold, to, slot=at)
        elif j == 1:
            push("ez", (i, j), ends, own_end, to, slot=at)
        else:
            push("ez", (i, j), folds, own_fold, to, slot=at)

    def pass_w(i, j):
        k = line[j] * 2 + y
        slot = wmain.at[i, k]
        copy("wz", (i, j), slot, slot, pair).wait_recv()
        wy[i, j] = push("wy", (i, j), slot, slot, across)
        for flag, ref in ((inner, wend.at[i, k]), (outer, wfold.at[i, k])):
            pl.when(flag)(copy("ez", (i, j), ref, ref, pair).wait_recv)
            push_if(flag, "ey", (i, j), ref, ref, across)

    def pass_pair(q):
        az[q].wait_recv()
        ax[1, q] = push("ax", (1, q), pair_act[q], pair_act[q], x_dev)
        ac[1, q] = push("ac", (1, q), pair_act[q], pair_act[q], twin)

    def pass_x(way, q):
        ax[way, q].wait_recv()
        ref = (x_act, xp_act)[way][q]
        ac[2 + way, q] = push("ac", (2 + way, q), ref, ref, twin)

    def multiply(i, zz, b, halves, fresh):
        a = 1 if i == 0 else 0
        product = 0.0
        for half in halves:
            k = 2 * zz + half
            product = product + dot(abuf[a, b, k], weight(i, k), 0, 0)
        if fresh:
            tot[i, b, 8:, :] = product
        else:
            tot[i, b, 8:, :] = tot[i, b, 8:, :] + product

    arrived, acts_seen = set(), set()

    def compute(i, j, which, *only):
        halves = only or (0, 1)
        if (i, j) not in arrived:
            arrived.add((i, j))
            wy[i, j].wait_recv()
            zz = z if j == 3 else line[j]
            k = zz * 2 + 1 - y

            @pl.when(inner)
            def _():
                copy("ey", (i, j), wend.at[i, k], wend.at[i, k], across).wait_recv()

            @pl.when(outer)
            def _():
                copy("ey", (i, j), wfold.at[i, k], wfold.at[i, k], across).wait_recv()
                unfold(i, k)
                if j != 3:
                    unfold(i, zz * 2 + y)

        for q in [half + (2 if i else 0) for half in halves]:
            for s in (0, 2) if which == 0 else (1, 3):
                if (s, q) not in acts_seen:
                    acts_seen.add((s, q))
                    ac[s, q].wait_recv()
        fresh = j == 3 and halves[0] == 0
        multiply(i, z if j == 3 else line[j], l if which == 0 else 1 - l, halves, fresh)

    sending = (
        "a0 a1 w03 w02", "w01 w13 a2 w00", "w12 w11 w23 a3", "w22 w21 w10 w20",
    )
    for item in " ".join(sending).split():
        if item[0] == "a":
            send_act(int(item[1]))
        else:
            send_w(int(item[1]), int(item[2]))
    passing = (
        "x00 w01 p0 x01", "c030 x02 w02 p1", "c010 x03 w11 c130", "c230 x10 p2 c020",
        "w12 x11 c110 c031", "w00 c011 w21 x12", "c120 c021 c1310 c1110", "p3 w22 c2310 c1210",
        "c000 c001 w10 c210", "c2110 x13 c220 c1311", "c1111 w20 c1211 c100", "c101",
    )
    for item in " ".join(passing).split():
        at = [int(v) for v in item[1:]]
        dict(x=pass_x, w=pass_w, p=pass_pair, c=compute)[item[0]](*at)
    for b in range(2):
        edge, where = tot.at[1, b, pl.ds(rows, 8)], m["halo_up"]
        if b == 0:
            push("hu", (0,), edge, where.at[y], across, slot=(y,))
        else:
            hu_near = copy("hu", (1,), edge, where.at[1], across)
            hu_far = copy("hu", (1,), edge, where.at[0], {"fs": zo * 2}, slot=(0,))
            pl.when(y == 0)(hu_near.start)
            pl.when(jnp.logical_and(y == 1, upper == 0))(hu_far.start)

    span = 32
    steps = rows // span

    def row(k):
        return tb[k : k + 1, :]

    def gelu_rows(b, r):
        at = pl.multiple_of(r * span, span)
        around = rounded(tot[1, b, pl.ds(at, span + 8), :])
        value = row(3) + row(0) * around[6 : 6 + span]
        value = value + row(1) * around[7 : 7 + span] + row(2) * around[8 : 8 + span]
        cdf = 0.5 * (1.0 + lax.erf(value * (1.0 / math.sqrt(2.0))))
        density = jnp.exp(-0.5 * value * value) * (1.0 / math.sqrt(2.0 * math.pi))
        hidden = rounded(tot[0, b, pl.ds(at + 8, span), :])
        dup[1, b, pl.ds(at, span), :] = (hidden * (value * cdf)).astype(jnp.bfloat16)
        dcv[b, pl.ds(at, span), :] = hidden * (cdf + value * density)

    @pl.loop(0, 2 * (steps - 1))
    def _(k):
        gelu_rows(lax.rem(k, 2), 1 + k // 2)

    compute(2, 3, 1, 1)
    compute(2, 1, 1, 1)
    compute(2, 2, 1)
    has_before = jnp.logical_or(y == 1, upper == 1)
    wait_up = [copy("hu", (b,), m["halo_up"].at[b], m["halo_up"].at[b], across) for b in range(2)]
    wait_up[1].wait_recv()
    pl.when(has_before)(wait_up[0].wait_recv)
    tot[1, 1, 0:8, :] = m["halo_up"][1]

    @pl.when(has_before)
    def _():
        tot[1, 0, 0:8, :] = m["halo_up"][0]

    @pl.when(jnp.logical_not(has_before))
    def _():
        tot[1, 0, 0:8, :] = jnp.zeros((8, ca), jnp.float32)

    @pl.loop(0, 2)
    def _(b):
        gelu_rows(b, 0)

    for which in range(2):
        compute(2, 0, which)

    def grad_rows(b, r, sums):
        at = pl.multiple_of(r * span, span)
        grad = dcv[b, pl.ds(at, span), :] * rounded(tot[2, b, pl.ds(at + 8, span), :])
        dcv[b, pl.ds(at, span), :] = grad
        around = rounded(tot[1, b, pl.ds(at, span + 8), :])

        def folded(value):
            total = value[0:8]
            for k in range(8, span, 8):
                total = total + value[k : k + 8]
            return total

        terms = [folded(grad * around[6 + i : 6 + i + span]) for i in range(3)] + [folded(grad)]
        return tuple(s + v for s, v in zip(sums, terms))

    sums = tuple(jnp.zeros((8, ca), jnp.float32) for _ in range(4))
    sums = lax.fori_loop(0, 2, lambda b, s: grad_rows(b, 0, s), sums)
    edge = dcv.at[0, pl.ds(0, 8)]
    hd_near = copy("hd", (0,), edge, m["halo_dc"].at[0], across)
    hd_far = copy("hd", (0,), edge, m["halo_dc"].at[1], {"fs": zo * 2 + 1}, slot=(1,))
    pl.when(y == 1)(hd_near.start)
    pl.when(jnp.logical_and(y == 0, upper == 1))(hd_far.start)
    push("hd", (1,), dcv.at[1, pl.ds(0, 8)], m["halo_dc"].at[y], across, slot=(y,))
    sums = lax.fori_loop(
        0, 2 * (steps - 1), lambda k, s: grad_rows(lax.rem(k, 2), 1 + k // 2, s), sums
    )
    m["col_own"][4:8, :] = jnp.zeros((4, ca), jnp.float32)
    for k in range(4):
        m["col_own"][k : k + 1, :] = jnp.sum(sums[k], axis=0, keepdims=True)
    group = [across, {"fs": zo * 2 + y}, {"fs": zo * 2 + 1 - y}]
    c1 = [push("c1", (k,), m["col_own"], m["col_got"].at[k], group[k]) for k in range(3)]

    def shift_rows(b, r):
        at = pl.multiple_of(r * span, span)
        ahead = dcv[b, pl.ds(at, span + 8), :]
        total = row(0) * ahead[2 : 2 + span] + row(1) * ahead[1 : 1 + span]
        total = total + row(2) * ahead[0:span]
        dup[0, b, pl.ds(at, span), :] = total.astype(jnp.bfloat16)

    @pl.loop(0, 2 * (steps - 1))
    def _(k):
        shift_rows(lax.rem(k, 2), k // 2)

    has_next = jnp.logical_or(y == 0, upper == 0)
    wait_dc = [copy("hd", (b,), m["halo_dc"].at[b], m["halo_dc"].at[b], across) for b in range(2)]
    wait_dc[0].wait_recv()
    pl.when(has_next)(wait_dc[1].wait_recv)
    dcv[0, rows : rows + 8, :] = m["halo_dc"][0]

    @pl.when(has_next)
    def _():
        dcv[1, rows : rows + 8, :] = m["halo_dc"][1]

    @pl.when(jnp.logical_not(has_next))
    def _():
        dcv[1, rows : rows + 8, :] = jnp.zeros((8, ca), jnp.float32)

    @pl.loop(0, 2)
    def _(b):
        shift_rows(b, steps - 1)

    def weight_grad(zz, yy):
        k = 2 * zz + yy
        return dot(abuf[0, 0, k], dup[0, 0], 1, 0) + dot(abuf[0, 1, k], dup[0, 1], 1, 0)

    def input_grad(b, k):
        return dot(weight(1, k), dup[0, b], 1, 1) + dot(weight(2, k), dup[1, b], 1, 1)

    b16, f32 = jnp.bfloat16, jnp.float32
    order = [far, zo, zp, z]
    ysend, yrecv, gown, zsend, zrecv = (m[k] for k in ("ysend", "yrecv", "gown", "zsend", "zrecv"))
    csend, crecv, pown, xsend, xrecv = (m[k] for k in ("csend", "crecv", "pown", "xsend", "xrecv"))
    psend, precv = m["psend"], m["precv"]
    gy, pc, px, pz = {}, {}, {}, {}

    def spot(bi, xi, half):
        return bi * 4 + xi * 2 + half

    def to_twin(bi, xi, half):
        b, xx, at = (1 - l, l)[bi], (1 - x, x)[xi], spot(bi, xi, half)
        csend[at] = input_grad(b, 2 * (xx * 2 + 1 - c) + half).astype(b16)
        pc[at] = push("pc", (at,), csend.at[at], crecv.at[at], twin)

    def keep(bi, xi, half):
        b, xx, at = (1 - l, l)[bi], (1 - x, x)[xi], spot(bi, xi, half)
        pown[at] = input_grad(b, 2 * (xx * 2 + c) + half)

    first_rows = -(-shard // 16) * 8
    parts = (pl.ds(0, first_rows), pl.ds(first_rows, shard - first_rows))

    def to_x(bi, half):
        at, to = spot(bi, 0, half), bi * 2 + half
        pc[at].wait_recv()
        for s, r in enumerate(parts):
            xsend[to, r, :] = (pown[at, r, :] + crecv[at, r, :].astype(f32)).astype(b16)
            px[to, s] = push("px", (to, s), xsend.at[to, r], xrecv.at[to, r], x_dev)

    def to_pair(half, s):
        at, r = spot(0, 1, half), parts[s]
        if s == 0:
            pc[at].wait_recv()
        px[half, s].wait_recv()
        total = pown[at, r, :] + crecv[at, r, :].astype(f32) + xrecv[half, r, :].astype(f32)
        psend[half, r, :] = total.astype(b16)
        pz[half, s] = push("pz", (half, s), psend.at[half, r], precv.at[half, r], pair)

    i_v, g_v, norm_v, taps_w, bias_w = (
        m[k] for k in ("i_v", "g_v", "norm_v", "taps_w", "bias_w")
    )
    stores = []

    def store(src, dst):
        made = pltpu.make_async_copy(src, dst, m["st"].at[len(stores)])
        made.start()
        stores.append(made)

    def finish(half):
        at = spot(1, 1, half)
        pc[at].wait_recv()
        for s, r in enumerate(parts):
            px[2 + half, s].wait_recv()
            pz[half, s].wait_recv()
            total = pown[at, r, :] + crecv[at, r, :].astype(f32)
            total = total + xrecv[2 + half, r, :].astype(f32) + precv[half, r, :].astype(f32)
            i_v[half, r, :] = total.astype(b16)
            store(i_v.at[half, r], outs[0].at[half, r])

    first_to = inner_i * zo + (1 - inner_i) * far
    first_at = 3 - 2 * inner_i
    last_at = 2 - inner_i

    def to_across(k):
        ysend[k] = weight_grad(order[k], 1 - y).astype(b16)
        for s, at in enumerate(parts):
            gy[k, s] = push("gy", (k, s), ysend.at[k, at], yrecv.at[k, at], across)

    def own(k):
        gown[k] = weight_grad(order[k], y)

    def add_across(k, s):
        gy[k, s].wait_recv()
        at = parts[s]
        gown[k, at, :] = gown[k, at, :] + yrecv[k, at, :].astype(f32)

    def to_line(k, s, dev, slot):
        at = parts[s]
        push(
            "gz", (k, s), zsend.at[k, at], zrecv.at[slot, at], {"fs": dev * 2 + y}, slot=(slot, s)
        )

    def got_line(k, s):
        at = parts[s]
        copy("gz", (k, s), zrecv.at[k, at], zrecv.at[k, at], across).wait_recv()

    def send_columns():
        for k in range(3):
            c1[k].wait_recv()
        got = m["col_got"]
        m["col_sum"][...] = (m["col_own"][...] + got[0]) + (got[1] + got[2])
        place = m["col_all"].at[mine, 1 - inner_i]
        place[...] = m["col_sum"][...]
        for k in range(1, 2 * t):
            tp = lax.rem(mine + k // 2, t)
            to = {"fs": (zp if k % 2 else z) * 2 + y, "tp": tp}
            c2.append(push("c2", (k - 1,), m["col_sum"], place, to))

    early, c2 = list(started), []
    to_across(0)
    to_twin(0, 0, 0)
    to_across(1)
    to_twin(0, 0, 1)
    keep(0, 0, 0)
    send_columns()
    to_x(0, 0)
    keep(0, 0, 1)
    to_x(0, 1)
    to_across(2)
    to_across(3)
    def to_other_half(k, s):
        add_across(k, s)
        zsend[k, parts[s], :] = gown[k, parts[s], :].astype(b16)
        if k == 0:
            to_line(0, s, first_to, first_at)
        else:
            to_line(1, s, zo, 0)

    own(0)
    to_other_half(0, 0)
    to_twin(0, 1, 0)
    to_twin(0, 1, 1)
    keep(0, 1, 0)
    to_other_half(0, 1)
    keep(0, 1, 1)
    own(1)
    to_pair(0, 0)
    to_twin(1, 0, 0)
    to_other_half(1, 0)
    to_twin(1, 0, 1)
    to_pair(0, 1)
    keep(1, 0, 0)
    to_x(1, 0)
    to_other_half(1, 1)
    keep(1, 0, 1)
    to_x(1, 1)
    own(2)
    for s in range(2):
        add_across(2, s)

        @pl.when(outer)
        def _(at=parts[s]):
            zsend[2, at, :] = gown[2, at, :].astype(b16)

        @pl.when(inner)
        def _(s=s, at=parts[s]):
            got_line(1, s)
            zsend[2, at, :] = (gown[2, at, :] + zrecv[1, at, :].astype(f32)).astype(b16)

        to_line(2, s, zp, last_at)
    to_pair(1, 0)
    to_pair(1, 1)
    own(3)
    for half in range(2):
        to_twin(1, 1, half)
        keep(1, 1, half)
    for s in range(2):
        add_across(3, s)
        got_line(0, s)
    norm_own, norm_all = m["norm_own"], m["norm_all"]
    norm_own[...] = jnp.zeros(norm_own.shape, f32)

    def settle(k, value):
        g_v[:, k * ca : k * ca + (cb if k else ca)] = value[:, : (cb if k else ca)]
        norm_own[k : k + 1, :] = jnp.sum(value * value, axis=0, keepdims=True)

    @pl.when(inner)
    def _():
        settle(0, gown[3] + zrecv[0].astype(f32))
        for s in range(2):
            got_line(2, s)
            got_line(3, s)
        settle(1, zrecv[2].astype(f32) + zrecv[3].astype(f32))

    @pl.when(outer)
    def _():
        settle(1, gown[3] + zrecv[0].astype(f32))
        for s in range(2):
            got_line(1, s)
        settle(0, zrecv[1].astype(f32))

    norms = [
        push("nm", (k,), norm_own, norm_all.at[me], others[k]) for k in range(n - 1)
    ]
    store(g_v, outs[1])
    for made in early:
        made.wait_send()
    for flag, made in guarded:
        pl.when(flag)(made.wait_send)
    finish(0)
    for copy_in in c2:
        copy_in.wait_recv()
    whole = m["col_all"]
    for p in range(t):
        at = p * width
        taps_w[:, at : at + ca] = whole[p, 0, 0:3, :]
        taps_w[:, at + ca : at + width] = whole[p, 1, 0:3, :cb]
        bias_w[at : at + ca] = whole[p, 0, 3, :]
        bias_w[at + ca : at + width] = whole[p, 1, 3, :cb]
    store(taps_w, outs[3])
    store(bias_w, outs[4])
    finish(1)
    for copy_in in norms:
        copy_in.wait_recv()
    norm_all[me] = norm_own[...]
    total = norm_all[0]
    for k in range(1, n):
        total = total + norm_all[k]
    norm_v[:ca] = total[0]
    norm_v[ca:] = total[1, :cb]
    store(norm_v, outs[2])
    for made in started[len(early) :]:
        made.wait_send()
    for made in stores:
        made.wait()
    pl.when(y == 0)(hu_near.wait_send)
    pl.when(jnp.logical_and(y == 1, upper == 0))(hu_far.wait_send)
    pl.when(y == 1)(hd_near.wait_send)
    pl.when(jnp.logical_and(y == 0, upper == 1))(hd_far.wait_send)


def publish_kernel(n, *refs):
    src, dst, held, sem = refs[:n], refs[n : 2 * n], refs[2 * n : 3 * n], refs[3 * n]
    into = [pltpu.make_async_copy(src[k], held[k], sem.at[0, k]) for k in range(n)]
    out = [pltpu.make_async_copy(held[k], dst[k], sem.at[1, k]) for k in range(n)]
    for made in into:
        made.start()
    for k in range(n):
        into[k].wait()
        out[k].start()
    for made in out:
        made.wait()


def publish(*arrays):
    n = len(arrays)
    return pl.pallas_call(
        functools.partial(publish_kernel, n),
        out_shape=[jax.ShapeDtypeStruct(v.shape, v.dtype) for v in arrays],
        in_specs=[ANY] * n,
        out_specs=[ANY] * n,
        scratch_shapes=[pltpu.VMEM(v.shape, v.dtype) for v in arrays]
        + [pltpu.SemaphoreType.DMA((2, n))],
        compiler_params=pltpu.CompilerParams(vmem_limit_bytes=VMEM_BYTES),
        name="publish",
    )(*arrays)


def with_kernel(inputs, w_conv_up, w_gate_up, w_down, taps, conv_bias, cotangent):
    n, t = lax.axis_size("fs"), lax.axis_size("tp")
    rows = inputs.shape[0]
    shard, width = w_conv_up.shape
    ca = -(-width // (2 * LANES)) * LANES
    shape = jax.ShapeDtypeStruct
    scratch = {**buffers(n, t, shard, width, rows, ca), **semaphores(n, t)}
    acts = [v.T.reshape(2, shard, rows) for v in (inputs, cotangent)]
    got = pl.pallas_call(
        functools.partial(layer_kernel, n, t, tuple(scratch)),
        out_shape=[
            shape((2, shard, rows), jnp.bfloat16),
            shape((shard, width), jnp.float32),
            shape((width,), jnp.float32),
            shape((TAPS, t * width), jnp.float32),
            shape((t * width,), jnp.float32),
        ],
        in_specs=[ANY] * 7,
        out_specs=[ANY] * 5,
        scratch_shapes=list(scratch.values()),
        compiler_params=pltpu.CompilerParams(
            collective_id=0, has_side_effects=True, vmem_limit_bytes=VMEM_BYTES
        ),
        name="layer",
    )(w_down.T, w_conv_up, w_gate_up, *acts, taps, conv_bias)
    grad_inputs, *others = publish(*got)
    return (grad_inputs.reshape(-1, rows).T, *others)


def per_device(inputs, w_conv_up, *rest):
    n, t = lax.axis_size("fs"), lax.axis_size("tp")
    shard, width = w_conv_up.shape
    rows, features = inputs.shape
    fits = n == 8 and t == 4 and features == 2 * shard
    aligned = shard % 8 == 0 and rows % LANES == 0 and width > 2 * LANES
    aligned = aligned and width % (2 * LANES) == LANES + LANES // 2
    chosen = with_kernel if fits and aligned else with_collectives
    return chosen(inputs, w_conv_up, *rest)


def solution(mesh):
    return jax.shard_map(
        per_device,
        mesh=mesh,
        in_specs=(
            P("fs", "tp"),
            P("fs", "tp"),
            P("fs", "tp"),
            P("tp", "fs"),
            P(),
            P(),
            P("fs", "tp"),
        ),
        out_specs=(P("fs", "tp"), P("fs", "tp"), P("tp"), P(), P()),
        check_vma=False,
    )
```

```python
import functools
import math

import jax
import jax.numpy as jnp
from jax import lax
from jax.experimental import pallas as pl
from jax.experimental.pallas import tpu as pltpu
from jax.sharding import PartitionSpec as P

TAPS = 3
LANES = 128
MESH = pl.DeviceIdType.MESH
VMEM_BYTES = 63 * 1024 * 1024
ANY = pl.BlockSpec(memory_space=pl.ANY)


def shifted(block, axis, distance):
    devices = range(lax.axis_size(axis))
    route = [(i - distance, i) for i in devices if i - distance in devices]
    return lax.ppermute(block, axis, route)


def gelu_parts(value):
    normal_cdf = 0.5 * (1.0 + jax.scipy.special.erf(value / math.sqrt(2.0)))
    density = jnp.exp(-0.5 * value * value) / math.sqrt(2.0 * math.pi)
    return (value * normal_cdf, normal_cdf + value * density)


def with_collectives(inputs, w_conv_up, w_gate_up, w_down, taps, conv_bias, cotangent):
    span = TAPS - 1
    rows = inputs.shape[0]
    width = w_conv_up.shape[1]
    col_start = lax.axis_index("tp") * width
    taps_own = lax.dynamic_slice_in_dim(taps, col_start, width, 1)
    bias_own = lax.dynamic_slice_in_dim(conv_bias, col_start, width, 0)
    features, cot_full = (
        lax.all_gather(inputs, "tp", axis=1, tiled=True),
        lax.all_gather(cotangent, "tp", axis=1, tiled=True),
    )
    conv_weight, gate_weight = (
        lax.all_gather(w_conv_up, "fs", axis=0, tiled=True),
        lax.all_gather(w_gate_up, "fs", axis=0, tiled=True),
    )
    columns = cot_full
    d_hidden = lax.dot_general(
        columns,
        lax.all_gather(w_down, "fs", axis=1, tiled=True),
        (((1,), (1,)), ((), ())),
        preferred_element_type=jnp.float32,
    ).astype(jnp.bfloat16)
    up_a = jnp.dot(features, conv_weight, preferred_element_type=jnp.float32).astype(jnp.bfloat16)
    up_b = jnp.dot(features, gate_weight, preferred_element_type=jnp.float32).astype(jnp.bfloat16)
    earlier = shifted(up_a[rows - span :], "fs", 1)
    extended = jnp.concatenate([earlier, up_a], 0).astype(jnp.float32)
    conv_out = bias_own[None, :] + sum(
        (taps_own[i][None, :] * extended[i : i + rows] for i in range(TAPS))
    )
    gelu_value, gelu_slope = gelu_parts(conv_out)
    hidden_grad = d_hidden.astype(jnp.float32)
    d_conv = hidden_grad * up_b.astype(jnp.float32) * gelu_slope
    d_up_b = (hidden_grad * gelu_value).astype(jnp.bfloat16)
    later = shifted(d_conv[:span], "fs", -1)
    d_extended = jnp.concatenate([d_conv, later], 0)
    d_up_a = sum(
        (taps_own[i][None, :] * d_extended[span - i : span - i + rows] for i in range(TAPS))
    ).astype(jnp.bfloat16)
    tap_terms = [jnp.sum(d_conv * extended[i : i + rows], axis=0) for i in range(TAPS)]
    column_part = jnp.stack(tap_terms + [jnp.sum(d_conv, axis=0)], 0)
    contract = (((1,), (1,)), ((), ()))
    partial_sum = lax.dot_general(d_up_a, conv_weight, contract, preferred_element_type=jnp.float32)
    partial_sum = partial_sum + lax.dot_general(
        d_up_b, gate_weight, contract, preferred_element_type=jnp.float32
    )
    grad_inputs = lax.psum_scatter(
        partial_sum.astype(jnp.bfloat16), "tp", scatter_dimension=1, tiled=True
    )
    columns = features
    grad_conv_up = lax.psum_scatter(
        lax.dot_general(
            columns, d_up_a, (((0,), (0,)), ((), ())), preferred_element_type=jnp.float32
        ),
        "fs",
        scatter_dimension=0,
        tiled=True,
    )
    squares = jnp.sum(grad_conv_up * grad_conv_up, axis=0)
    placed = jnp.zeros((TAPS + 1, width * lax.axis_size("tp")), jnp.float32)
    placed = lax.dynamic_update_slice_in_dim(placed, column_part, col_start, 1)
    full_columns = lax.psum(placed, ("fs", "tp"))
    unit_norms = lax.psum(squares, "fs")
    return (grad_inputs, grad_conv_up, unit_norms, full_columns[:TAPS], full_columns[TAPS])


def greet(peers):
    barrier = pltpu.get_barrier_semaphore()
    for peer in peers:
        pl.semaphore_signal(barrier, inc=1, device_id=peer, device_id_type=MESH)


def greeted(peers):
    pl.semaphore_wait(pltpu.get_barrier_semaphore(), len(peers))


def dot(a, b, da, db):
    return lax.dot_general(
        a, b, (((da,), (db,)), ((), ())), preferred_element_type=jnp.float32
    )


def rounded(value):
    return value.astype(jnp.bfloat16).astype(jnp.float32)


def folded_rows(rows):
    return -(-rows // 32) * 16


def buffers(n, t, shard, width, rows, ca):
    b16, f32 = jnp.bfloat16, jnp.float32
    full, fold = ca // LANES - 1, folded_rows(shard)
    return dict(
        wv=pltpu.VMEM((3, shard, width), b16),
        taps_v=pltpu.VMEM((TAPS, t * width), f32),
        bias_v=pltpu.VMEM((t * width,), f32),
        i_v=pltpu.VMEM((2, shard, rows), b16),
        g_v=pltpu.VMEM((shard, width), f32),
        norm_v=pltpu.VMEM((width,), f32),
        taps_w=pltpu.VMEM((TAPS, t * width), f32),
        bias_w=pltpu.VMEM((t * width,), f32),
        stage=pltpu.VMEM((2, 3, full, shard, LANES), b16),
        stage_end=pltpu.VMEM((3, shard, LANES), b16),
        stage_fold=pltpu.VMEM((3, fold, LANES), b16),
        wmain=pltpu.VMEM((3, n, full, shard, LANES), b16),
        wend=pltpu.VMEM((3, n, shard, LANES), b16),
        wfold=pltpu.VMEM((3, n, fold, LANES), b16),
        abuf=pltpu.VMEM((2, 2, n, shard, rows), b16),
        tot=pltpu.VMEM((3, 2, rows + 8, ca), f32),
        halo_up=pltpu.VMEM((2, 8, ca), f32),
        halo_dc=pltpu.VMEM((2, 8, ca), f32),
        tb=pltpu.VMEM((8, ca), f32),
        dcv=pltpu.VMEM((2, rows + 8, ca), f32),
        dup=pltpu.VMEM((2, 2, rows, ca), b16),
        col_own=pltpu.VMEM((8, ca), f32),
        col_got=pltpu.VMEM((3, 8, ca), f32),
        col_sum=pltpu.VMEM((8, ca), f32),
        col_all=pltpu.VMEM((t, 2, 8, ca), f32),
        ysend=pltpu.VMEM((4, shard, ca), b16),
        yrecv=pltpu.VMEM((4, shard, ca), b16),
        gown=pltpu.VMEM((4, shard, ca), f32),
        zsend=pltpu.VMEM((3, shard, ca), b16),
        zrecv=pltpu.VMEM((4, shard, ca), b16),
        csend=pltpu.VMEM((8, shard, rows), b16),
        crecv=pltpu.VMEM((8, shard, rows), b16),
        pown=pltpu.VMEM((8, shard, rows), f32),
        xsend=pltpu.VMEM((4, shard, rows), b16),
        xrecv=pltpu.VMEM((4, shard, rows), b16),
        psend=pltpu.VMEM((2, shard, rows), b16),
        precv=pltpu.VMEM((2, shard, rows), b16),
        norm_own=pltpu.VMEM((8, ca), f32),
        norm_all=pltpu.VMEM((n, 8, ca), f32),
    )


def semaphores(n, t):
    shapes = dict(
        wz=(3, 3), wy=(3, 4), ez=(3, 3), ey=(3, 4), az=(4,), ax=(2, 4), ac=(4, 4), hu=(2,), hd=(2,),
        c1=(3,), c2=(2 * t - 1,), gy=(4, 2), gz=(4, 2), pc=(8,), px=(4, 2), pz=(2, 2), nm=(n - 1,),
    )
    dma = pltpu.SemaphoreType.DMA
    local = dict(ld=dma((9,)), st=dma((8,)))
    return local | {name + end: dma(s) for name, s in shapes.items() for end in ("_s", "_r")}


def layer_kernel(n, t, names, *refs):
    w_in, acts, taps_in, bias_in = refs[:3], refs[3:5], refs[5], refs[6]
    outs = refs[7:12]
    m = dict(zip(names, refs[12:]))
    stage, stage_end, stage_fold = m["stage"], m["stage_end"], m["stage_fold"]
    wmain, wend, wfold, abuf, tot = m["wmain"], m["wend"], m["wfold"], m["abuf"], m["tot"]
    dcv, dup, tb = m["dcv"], m["dup"], m["tb"]
    w, taps, bias = m["wv"], m["taps_v"], m["bias_v"]
    shard, width = w.shape[1:]
    full, fold = stage.shape[2], stage_fold.shape[1]
    ca = (full + 1) * LANES
    cb = width - ca
    odd = cb - full * LANES
    rows = acts[0].shape[2]
    me, mine = lax.axis_index("fs"), lax.axis_index("tp")
    z, y = me // 2, lax.rem(me, 2)
    x, c = mine // 2, lax.rem(mine, 2)
    l = lax.rem(z, 2)
    upper = z // 2
    zp = z + 1 - 2 * l
    zo = 3 - z
    far = 3 - zp
    inner_i = lax.rem((z + 1) // 2, 2)
    inner = inner_i == 1
    outer = inner_i == 0
    across = {"fs": z * 2 + 1 - y}
    pair = {"fs": zp * 2 + y}
    x_dev = {"tp": (1 - x) * 2 + c}
    twin = {"tp": x * 2 + 1 - c}
    x_tp = (1 - x) * 2 + c
    line = [zp, 2 - upper, 3 * (1 - upper)]
    started, guarded = [], []

    def copy(name, at, src, dst, to, slot=None):
        slot = at if slot is None else slot
        return pltpu.make_async_remote_copy(
            src_ref=src, dst_ref=dst,
            send_sem=m[name + "_s"].at[at], recv_sem=m[name + "_r"].at[slot],
            device_id=to, device_id_type=MESH,
        )

    def push(*args, **kw):
        made = copy(*args, **kw)
        made.start()
        started.append(made)
        return made

    def push_if(flag, *args, **kw):
        made = copy(*args, **kw)
        pl.when(flag)(made.start)
        guarded.append((flag, made))

    def put(i):
        for k in range(full):
            at = k * LANES
            stage[0, i, k] = w[i, :, at : at + LANES]
            stage[1, i, k] = w[i, :, ca + at : ca + at + LANES]
        end = w[i, :, ca + full * LANES :]
        stage_end[i] = w[i, :, full * LANES : ca]
        stage_fold[i] = jnp.zeros((fold, LANES), jnp.bfloat16)
        stage_fold[i, :, :odd] = end[:fold]
        stage_fold[i, : shard - fold, odd:] = end[fold:]
        wmain[i, me] = stage[1 - inner_i, i]

        @pl.when(inner)
        def _():
            wend[i, me] = stage_end[i]

        @pl.when(outer)
        def _():
            wend[i, me] = jnp.zeros((shard, LANES), jnp.bfloat16)
            wend[i, me, :, :odd] = end

    def unfold(i, k):
        both = wfold[i, k].astype(jnp.float32)
        low = lax.broadcasted_iota(jnp.int32, both.shape, 1) < odd
        first = jnp.where(low, both, 0.0).astype(jnp.bfloat16)
        second = jnp.where(low, pltpu.roll(both, LANES - odd, 1), 0.0).astype(jnp.bfloat16)
        wend[i, k, :fold] = first
        wend[i, k, fold:] = second[: shard - fold]

    def weight(i, k):
        return jnp.concatenate([wmain[i, k, c] for c in range(full)] + [wend[i, k]], axis=1)

    others = [{"fs": lax.rem(me + k, n)} for k in range(1, n)]
    others += [{"tp": lax.rem(mine + k, t)} for k in range(1, t)]
    others += [{"fs": zp * 2 + y, "tp": lax.rem(mine + k, t)} for k in range(1, t)]
    greet(others)
    loads = []

    def load(src, dst):
        made = pltpu.make_async_copy(src, dst, m["ld"].at[len(loads)])
        made.start()
        loads.append(made)

    for i in range(3):
        load(w_in[i], w.at[i])
    for a in range(2):
        for half in range(2):
            load(acts[a].at[half], abuf.at[a, l, 2 * mine + half])
    load(taps_in, taps)
    load(bias_in, bias)
    for i in range(3):
        loads[i].wait()
        put(i)
    for made in loads[3:]:
        made.wait()
    tb[...] = jnp.zeros(tb.shape, jnp.float32)
    for p in range(t):
        for flag, start, size in ((inner, 0, ca), (outer, ca, cb)):
            @pl.when(jnp.logical_and(mine == p, flag))
            def _(p=p, start=start, size=size):
                at = p * width + start
                tb[0:3, 0:size] = taps[:, at : at + size]
                tb[3:4, 0:size] = bias[at : at + size].reshape(1, size)

    greeted(others)

    quarter = [(1, 0), (1, 1), (0, 0), (0, 1)]
    own_act = [abuf.at[a, l, 2 * mine + half] for a, half in quarter]
    pair_act = [abuf.at[a, 1 - l, 2 * mine + half] for a, half in quarter]
    x_act = [abuf.at[a, l, 2 * x_tp + half] for a, half in quarter]
    xp_act = [abuf.at[a, 1 - l, 2 * x_tp + half] for a, half in quarter]
    az, ax, ac, wz, wy = {}, {}, {}, {}, {}

    def send_act(q):
        az[q] = push("az", (q,), own_act[q], own_act[q], pair)
        ax[0, q] = push("ax", (0, q), own_act[q], own_act[q], x_dev)
        ac[0, q] = push("ac", (0, q), own_act[q], own_act[q], twin)

    def send_w(i, j):
        own, own_end, own_fold = wmain.at[i, me], wend.at[i, me], wfold.at[i, me]
        ends, folds = stage_end.at[i], stage_fold.at[i]
        if j == 3:
            wy[i, 3] = push("wy", (i, 3), own, own, across)
            push_if(inner, "ey", (i, 3), ends, own_end, across)
            push_if(outer, "ey", (i, 3), folds, own_fold, across)
            return
        to = {"fs": line[j] * 2 + y}
        at = (i, 0 if j == 0 else 2 - inner_i)
        push("wz", (i, j), stage.at[inner_i if j == 0 else j - 1, i], own, to, slot=at)
        if j == 0:
            push_if(outer, "ez", (i, j), ends, own_end, to, slot=at)
            push_if(inner, "ez", (i, j), folds, own_fold, to, slot=at)
        elif j == 1:
            push("ez", (i, j), ends, own_end, to, slot=at)
        else:
            push("ez", (i, j), folds, own_fold, to, slot=at)

    def pass_w(i, j):
        k = line[j] * 2 + y
        slot = wmain.at[i, k]
        copy("wz", (i, j), slot, slot, pair).wait_recv()
        wy[i, j] = push("wy", (i, j), slot, slot, across)
        for flag, ref in ((inner, wend.at[i, k]), (outer, wfold.at[i, k])):
            pl.when(flag)(copy("ez", (i, j), ref, ref, pair).wait_recv)
            push_if(flag, "ey", (i, j), ref, ref, across)

    def pass_pair(q):
        az[q].wait_recv()
        ax[1, q] = push("ax", (1, q), pair_act[q], pair_act[q], x_dev)
        ac[1, q] = push("ac", (1, q), pair_act[q], pair_act[q], twin)

    def pass_x(way, q):
        ax[way, q].wait_recv()
        ref = (x_act, xp_act)[way][q]
        ac[2 + way, q] = push("ac", (2 + way, q), ref, ref, twin)

    def multiply(i, zz, b, halves, fresh):
        a = 1 if i == 0 else 0
        product = 0.0
        for half in halves:
            k = 2 * zz + half
            product = product + dot(abuf[a, b, k], weight(i, k), 0, 0)
        if fresh:
            tot[i, b, 8:, :] = product
        else:
            tot[i, b, 8:, :] = tot[i, b, 8:, :] + product

    arrived, acts_seen = set(), set()

    def compute(i, j, which, *only):
        halves = only or (0, 1)
        if (i, j) not in arrived:
            arrived.add((i, j))
            wy[i, j].wait_recv()
            zz = z if j == 3 else line[j]
            k = zz * 2 + 1 - y

            @pl.when(inner)
            def _():
                copy("ey", (i, j), wend.at[i, k], wend.at[i, k], across).wait_recv()

            @pl.when(outer)
            def _():
                copy("ey", (i, j), wfold.at[i, k], wfold.at[i, k], across).wait_recv()
                unfold(i, k)
                if j != 3:
                    unfold(i, zz * 2 + y)

        for q in [half + (2 if i else 0) for half in halves]:
            for s in (0, 2) if which == 0 else (1, 3):
                if (s, q) not in acts_seen:
                    acts_seen.add((s, q))
                    ac[s, q].wait_recv()
        fresh = j == 3 and halves[0] == 0
        multiply(i, z if j == 3 else line[j], l if which == 0 else 1 - l, halves, fresh)

    sending = (
        "a0 a1 w03 w02", "w01 w13 a2 w00", "w12 w11 w23 a3", "w22 w21 w10 w20",
    )
    for item in " ".join(sending).split():
        if item[0] == "a":
            send_act(int(item[1]))
        else:
            send_w(int(item[1]), int(item[2]))
    passing = (
        "x00 w01 p0 x01", "c030 x02 w02 p1", "c010 x03 w11 c130", "c230 x10 p2 c020",
        "w12 x11 c110 c031", "w00 c011 w21 x12", "c120 c021 c1310 c1110", "p3 w22 c2310 c1210",
        "c000 c001 w10 c210", "c2110 x13 c220 c1311", "c1111 w20 c1211 c100", "c101",
    )
    for item in " ".join(passing).split():
        at = [int(v) for v in item[1:]]
        dict(x=pass_x, w=pass_w, p=pass_pair, c=compute)[item[0]](*at)
    for b in range(2):
        edge, where = tot.at[1, b, pl.ds(rows, 8)], m["halo_up"]
        if b == 0:
            push("hu", (0,), edge, where.at[y], across, slot=(y,))
        else:
            hu_near = copy("hu", (1,), edge, where.at[1], across)
            hu_far = copy("hu", (1,), edge, where.at[0], {"fs": zo * 2}, slot=(0,))
            pl.when(y == 0)(hu_near.start)
            pl.when(jnp.logical_and(y == 1, upper == 0))(hu_far.start)

    span = 32
    steps = rows // span

    def row(k):
        return tb[k : k + 1, :]

    def gelu_rows(b, r):
        at = pl.multiple_of(r * span, span)
        around = rounded(tot[1, b, pl.ds(at, span + 8), :])
        value = row(3) + row(0) * around[6 : 6 + span]
        value = value + row(1) * around[7 : 7 + span] + row(2) * around[8 : 8 + span]
        cdf = 0.5 * (1.0 + lax.erf(value * (1.0 / math.sqrt(2.0))))
        density = jnp.exp(-0.5 * value * value) * (1.0 / math.sqrt(2.0 * math.pi))
        hidden = rounded(tot[0, b, pl.ds(at + 8, span), :])
        dup[1, b, pl.ds(at, span), :] = (hidden * (value * cdf)).astype(jnp.bfloat16)
        dcv[b, pl.ds(at, span), :] = hidden * (cdf + value * density)

    @pl.loop(0, 2 * (steps - 1))
    def _(k):
        gelu_rows(lax.rem(k, 2), 1 + k // 2)

    compute(2, 3, 1, 1)
    compute(2, 1, 1, 1)
    compute(2, 2, 1)
    has_before = jnp.logical_or(y == 1, upper == 1)
    wait_up = [copy("hu", (b,), m["halo_up"].at[b], m["halo_up"].at[b], across) for b in range(2)]
    wait_up[1].wait_recv()
    pl.when(has_before)(wait_up[0].wait_recv)
    tot[1, 1, 0:8, :] = m["halo_up"][1]

    @pl.when(has_before)
    def _():
        tot[1, 0, 0:8, :] = m["halo_up"][0]

    @pl.when(jnp.logical_not(has_before))
    def _():
        tot[1, 0, 0:8, :] = jnp.zeros((8, ca), jnp.float32)

    @pl.loop(0, 2)
    def _(b):
        gelu_rows(b, 0)

    for which in range(2):
        compute(2, 0, which)

    def grad_rows(b, r, sums):
        at = pl.multiple_of(r * span, span)
        grad = dcv[b, pl.ds(at, span), :] * rounded(tot[2, b, pl.ds(at + 8, span), :])
        dcv[b, pl.ds(at, span), :] = grad
        around = rounded(tot[1, b, pl.ds(at, span + 8), :])

        def folded(value):
            total = value[0:8]
            for k in range(8, span, 8):
                total = total + value[k : k + 8]
            return total

        terms = [folded(grad * around[6 + i : 6 + i + span]) for i in range(3)] + [folded(grad)]
        return tuple(s + v for s, v in zip(sums, terms))

    sums = tuple(jnp.zeros((8, ca), jnp.float32) for _ in range(4))
    sums = lax.fori_loop(0, 2, lambda b, s: grad_rows(b, 0, s), sums)
    edge = dcv.at[0, pl.ds(0, 8)]
    hd_near = copy("hd", (0,), edge, m["halo_dc"].at[0], across)
    hd_far = copy("hd", (0,), edge, m["halo_dc"].at[1], {"fs": zo * 2 + 1}, slot=(1,))
    pl.when(y == 1)(hd_near.start)
    pl.when(jnp.logical_and(y == 0, upper == 1))(hd_far.start)
    push("hd", (1,), dcv.at[1, pl.ds(0, 8)], m["halo_dc"].at[y], across, slot=(y,))
    sums = lax.fori_loop(
        0, 2 * (steps - 1), lambda k, s: grad_rows(lax.rem(k, 2), 1 + k // 2, s), sums
    )
    m["col_own"][4:8, :] = jnp.zeros((4, ca), jnp.float32)
    for k in range(4):
        m["col_own"][k : k + 1, :] = jnp.sum(sums[k], axis=0, keepdims=True)
    group = [across, {"fs": zo * 2 + y}, {"fs": zo * 2 + 1 - y}]
    c1 = [push("c1", (k,), m["col_own"], m["col_got"].at[k], group[k]) for k in range(3)]

    def shift_rows(b, r):
        at = pl.multiple_of(r * span, span)
        ahead = dcv[b, pl.ds(at, span + 8), :]
        total = row(0) * ahead[2 : 2 + span] + row(1) * ahead[1 : 1 + span]
        total = total + row(2) * ahead[0:span]
        dup[0, b, pl.ds(at, span), :] = total.astype(jnp.bfloat16)

    @pl.loop(0, 2 * (steps - 1))
    def _(k):
        shift_rows(lax.rem(k, 2), k // 2)

    has_next = jnp.logical_or(y == 0, upper == 0)
    wait_dc = [copy("hd", (b,), m["halo_dc"].at[b], m["halo_dc"].at[b], across) for b in range(2)]
    wait_dc[0].wait_recv()
    pl.when(has_next)(wait_dc[1].wait_recv)
    dcv[0, rows : rows + 8, :] = m["halo_dc"][0]

    @pl.when(has_next)
    def _():
        dcv[1, rows : rows + 8, :] = m["halo_dc"][1]

    @pl.when(jnp.logical_not(has_next))
    def _():
        dcv[1, rows : rows + 8, :] = jnp.zeros((8, ca), jnp.float32)

    @pl.loop(0, 2)
    def _(b):
        shift_rows(b, steps - 1)

    def weight_grad(zz, yy):
        k = 2 * zz + yy
        return dot(abuf[0, 0, k], dup[0, 0], 1, 0) + dot(abuf[0, 1, k], dup[0, 1], 1, 0)

    def input_grad(b, k):
        return dot(weight(1, k), dup[0, b], 1, 1) + dot(weight(2, k), dup[1, b], 1, 1)

    b16, f32 = jnp.bfloat16, jnp.float32
    order = [far, zo, zp, z]
    ysend, yrecv, gown, zsend, zrecv = (m[k] for k in ("ysend", "yrecv", "gown", "zsend", "zrecv"))
    csend, crecv, pown, xsend, xrecv = (m[k] for k in ("csend", "crecv", "pown", "xsend", "xrecv"))
    psend, precv = m["psend"], m["precv"]
    gy, pc, px, pz = {}, {}, {}, {}

    def spot(bi, xi, half):
        return bi * 4 + xi * 2 + half

    def to_twin(bi, xi, half):
        b, xx, at = (1 - l, l)[bi], (1 - x, x)[xi], spot(bi, xi, half)
        csend[at] = input_grad(b, 2 * (xx * 2 + 1 - c) + half).astype(b16)
        pc[at] = push("pc", (at,), csend.at[at], crecv.at[at], twin)

    def keep(bi, xi, half):
        b, xx, at = (1 - l, l)[bi], (1 - x, x)[xi], spot(bi, xi, half)
        pown[at] = input_grad(b, 2 * (xx * 2 + c) + half)

    first_rows = -(-shard // 16) * 8
    parts = (pl.ds(0, first_rows), pl.ds(first_rows, shard - first_rows))

    def to_x(bi, half):
        at, to = spot(bi, 0, half), bi * 2 + half
        pc[at].wait_recv()
        for s, r in enumerate(parts):
            xsend[to, r, :] = (pown[at, r, :] + crecv[at, r, :].astype(f32)).astype(b16)
            px[to, s] = push("px", (to, s), xsend.at[to, r], xrecv.at[to, r], x_dev)

    def to_pair(half, s):
        at, r = spot(0, 1, half), parts[s]
        if s == 0:
            pc[at].wait_recv()
        px[half, s].wait_recv()
        total = pown[at, r, :] + crecv[at, r, :].astype(f32) + xrecv[half, r, :].astype(f32)
        psend[half, r, :] = total.astype(b16)
        pz[half, s] = push("pz", (half, s), psend.at[half, r], precv.at[half, r], pair)

    i_v, g_v, norm_v, taps_w, bias_w = (
        m[k] for k in ("i_v", "g_v", "norm_v", "taps_w", "bias_w")
    )
    stores = []

    def store(src, dst):
        made = pltpu.make_async_copy(src, dst, m["st"].at[len(stores)])
        made.start()
        stores.append(made)

    def finish(half):
        at = spot(1, 1, half)
        pc[at].wait_recv()
        for s, r in enumerate(parts):
            px[2 + half, s].wait_recv()
            pz[half, s].wait_recv()
            total = pown[at, r, :] + crecv[at, r, :].astype(f32)
            total = total + xrecv[2 + half, r, :].astype(f32) + precv[half, r, :].astype(f32)
            i_v[half, r, :] = total.astype(b16)
            store(i_v.at[half, r], outs[0].at[half, r])

    first_to = inner_i * zo + (1 - inner_i) * far
    first_at = 3 - 2 * inner_i
    last_at = 2 - inner_i

    def to_across(k):
        ysend[k] = weight_grad(order[k], 1 - y).astype(b16)
        for s, at in enumerate(parts):
            gy[k, s] = push("gy", (k, s), ysend.at[k, at], yrecv.at[k, at], across)

    def own(k):
        gown[k] = weight_grad(order[k], y)

    def add_across(k, s):
        gy[k, s].wait_recv()
        at = parts[s]
        gown[k, at, :] = gown[k, at, :] + yrecv[k, at, :].astype(f32)

    def to_line(k, s, dev, slot):
        at = parts[s]
        push(
            "gz", (k, s), zsend.at[k, at], zrecv.at[slot, at], {"fs": dev * 2 + y}, slot=(slot, s)
        )

    def got_line(k, s):
        at = parts[s]
        copy("gz", (k, s), zrecv.at[k, at], zrecv.at[k, at], across).wait_recv()

    def send_columns():
        for k in range(3):
            c1[k].wait_recv()
        got = m["col_got"]
        m["col_sum"][...] = (m["col_own"][...] + got[0]) + (got[1] + got[2])
        place = m["col_all"].at[mine, 1 - inner_i]
        place[...] = m["col_sum"][...]
        for k in range(1, 2 * t):
            tp = lax.rem(mine + k // 2, t)
            to = {"fs": (zp if k % 2 else z) * 2 + y, "tp": tp}
            c2.append(push("c2", (k - 1,), m["col_sum"], place, to))

    early, c2 = list(started), []
    to_across(0)
    to_twin(0, 0, 0)
    keep(0, 0, 0)
    to_twin(0, 0, 1)
    to_x(0, 0)
    to_across(1)
    keep(0, 0, 1)
    to_x(0, 1)
    send_columns()
    to_across(2)
    to_across(3)
    def to_other_half(k, s):
        add_across(k, s)
        zsend[k, parts[s], :] = gown[k, parts[s], :].astype(b16)
        if k == 0:
            to_line(0, s, first_to, first_at)
        else:
            to_line(1, s, zo, 0)

    own(0)
    to_other_half(0, 0)
    to_twin(0, 1, 0)
    to_twin(0, 1, 1)
    keep(0, 1, 0)
    to_other_half(0, 1)
    keep(0, 1, 1)
    own(1)
    to_pair(0, 0)
    to_twin(1, 0, 0)
    to_other_half(1, 0)
    to_twin(1, 0, 1)
    to_pair(0, 1)
    keep(1, 0, 0)
    to_x(1, 0)
    to_other_half(1, 1)
    keep(1, 0, 1)
    to_x(1, 1)
    own(2)
    for s in range(2):
        add_across(2, s)

        @pl.when(outer)
        def _(at=parts[s]):
            zsend[2, at, :] = gown[2, at, :].astype(b16)

        @pl.when(inner)
        def _(s=s, at=parts[s]):
            got_line(1, s)
            zsend[2, at, :] = (gown[2, at, :] + zrecv[1, at, :].astype(f32)).astype(b16)

        to_line(2, s, zp, last_at)
    to_pair(1, 0)
    to_pair(1, 1)
    own(3)
    for half in range(2):
        to_twin(1, 1, half)
        keep(1, 1, half)
    for s in range(2):
        add_across(3, s)
        got_line(0, s)
    norm_own, norm_all = m["norm_own"], m["norm_all"]
    norm_own[...] = jnp.zeros(norm_own.shape, f32)

    def settle(k, value):
        g_v[:, k * ca : k * ca + (cb if k else ca)] = value[:, : (cb if k else ca)]
        norm_own[k : k + 1, :] = jnp.sum(value * value, axis=0, keepdims=True)

    @pl.when(inner)
    def _():
        settle(0, gown[3] + zrecv[0].astype(f32))
        for s in range(2):
            got_line(2, s)
            got_line(3, s)
        settle(1, zrecv[2].astype(f32) + zrecv[3].astype(f32))

    @pl.when(outer)
    def _():
        settle(1, gown[3] + zrecv[0].astype(f32))
        for s in range(2):
            got_line(1, s)
        settle(0, zrecv[1].astype(f32))

    norms = [
        push("nm", (k,), norm_own, norm_all.at[me], others[k]) for k in range(n - 1)
    ]
    store(g_v, outs[1])
    for made in early:
        made.wait_send()
    for flag, made in guarded:
        pl.when(flag)(made.wait_send)
    finish(0)
    for copy_in in c2:
        copy_in.wait_recv()
    whole = m["col_all"]
    for p in range(t):
        at = p * width
        taps_w[:, at : at + ca] = whole[p, 0, 0:3, :]
        taps_w[:, at + ca : at + width] = whole[p, 1, 0:3, :cb]
        bias_w[at : at + ca] = whole[p, 0, 3, :]
        bias_w[at + ca : at + width] = whole[p, 1, 3, :cb]
    store(taps_w, outs[3])
    store(bias_w, outs[4])
    finish(1)
    for copy_in in norms:
        copy_in.wait_recv()
    norm_all[me] = norm_own[...]
    total = norm_all[0]
    for k in range(1, n):
        total = total + norm_all[k]
    norm_v[:ca] = total[0]
    norm_v[ca:] = total[1, :cb]
    store(norm_v, outs[2])
    for made in started[len(early) :]:
        made.wait_send()
    for made in stores:
        made.wait()
    pl.when(y == 0)(hu_near.wait_send)
    pl.when(jnp.logical_and(y == 1, upper == 0))(hu_far.wait_send)
    pl.when(y == 1)(hd_near.wait_send)
    pl.when(jnp.logical_and(y == 0, upper == 1))(hd_far.wait_send)


def publish_kernel(n, *refs):
    src, dst, held, sem = refs[:n], refs[n : 2 * n], refs[2 * n : 3 * n], refs[3 * n]
    into = [pltpu.make_async_copy(src[k], held[k], sem.at[0, k]) for k in range(n)]
    out = [pltpu.make_async_copy(held[k], dst[k], sem.at[1, k]) for k in range(n)]
    for made in into:
        made.start()
    for k in range(n):
        into[k].wait()
        out[k].start()
    for made in out:
        made.wait()


def publish(*arrays):
    n = len(arrays)
    return pl.pallas_call(
        functools.partial(publish_kernel, n),
        out_shape=[jax.ShapeDtypeStruct(v.shape, v.dtype) for v in arrays],
        in_specs=[ANY] * n,
        out_specs=[ANY] * n,
        scratch_shapes=[pltpu.VMEM(v.shape, v.dtype) for v in arrays]
        + [pltpu.SemaphoreType.DMA((2, n))],
        compiler_params=pltpu.CompilerParams(vmem_limit_bytes=VMEM_BYTES),
        name="publish",
    )(*arrays)


def with_kernel(inputs, w_conv_up, w_gate_up, w_down, taps, conv_bias, cotangent):
    n, t = lax.axis_size("fs"), lax.axis_size("tp")
    rows = inputs.shape[0]
    shard, width = w_conv_up.shape
    ca = -(-width // (2 * LANES)) * LANES
    shape = jax.ShapeDtypeStruct
    scratch = {**buffers(n, t, shard, width, rows, ca), **semaphores(n, t)}
    acts = [v.T.reshape(2, shard, rows) for v in (inputs, cotangent)]
    got = pl.pallas_call(
        functools.partial(layer_kernel, n, t, tuple(scratch)),
        out_shape=[
            shape((2, shard, rows), jnp.bfloat16),
            shape((shard, width), jnp.float32),
            shape((width,), jnp.float32),
            shape((TAPS, t * width), jnp.float32),
            shape((t * width,), jnp.float32),
        ],
        in_specs=[ANY] * 7,
        out_specs=[ANY] * 5,
        scratch_shapes=list(scratch.values()),
        compiler_params=pltpu.CompilerParams(
            collective_id=0, has_side_effects=True, vmem_limit_bytes=VMEM_BYTES
        ),
        name="layer",
    )(w_down.T, w_conv_up, w_gate_up, *acts, taps, conv_bias)
    grad_inputs, *others = publish(*got)
    return (grad_inputs.reshape(-1, rows).T, *others)


def per_device(inputs, w_conv_up, *rest):
    n, t = lax.axis_size("fs"), lax.axis_size("tp")
    shard, width = w_conv_up.shape
    rows, features = inputs.shape
    fits = n == 8 and t == 4 and features == 2 * shard
    aligned = shard % 8 == 0 and rows % LANES == 0 and width > 2 * LANES
    aligned = aligned and width % (2 * LANES) == LANES + LANES // 2
    chosen = with_kernel if fits and aligned else with_collectives
    return chosen(inputs, w_conv_up, *rest)


def solution(mesh):
    return jax.shard_map(
        per_device,
        mesh=mesh,
        in_specs=(
            P("fs", "tp"),
            P("fs", "tp"),
            P("fs", "tp"),
            P("tp", "fs"),
            P(),
            P(),
            P("fs", "tp"),
        ),
        out_specs=(P("fs", "tp"), P("fs", "tp"), P("tp"), P(), P()),
        check_vma=False,
    )
```
